256 devices in a mesh: grp: 2 (over y), ep: 32 (over z, core), tp: 4 (over x).
Axes of the slice: x: 4, y: 2, z: 16, core: 2. Of those that a mesh axis runs over, the one named last changes fastest.
The devices are a block of a 4x16x16 slice.
Arguments:
- x_in: bfloat16 [4096, 2048], P(('grp', 'ep')), parts along dimension 0, may hold values from -6 to 6
- state: float32 [4096, 96, 128], P(('grp', 'ep'), 'tp'), parts along dimension 0, may hold values from -6 to 6
- routes: int32 [4096, 2], P(('grp', 'ep')), parts along dimension 0, may hold values from 0 to 63, as said below
- w_in: bfloat16 [2048, 1536], P(None, 'tp'), may hold values from -0.125 to 0.125
- decay_rate: float32 [96, 64], P('tp'), may hold values from 0.01 to 1
- frequency: float32 [96, 64], P('tp'), may hold values from 0 to 192
- log_step: float32 [96], P('tp'), may hold values from -3 to 0
- b_in: float32 [96, 16, 128], P('tp'), may hold values from -1.5 to 1.5
- c_out: float32 [96, 16, 128], P('tp'), may hold values from -0.5 to 0.5
- skip: float32 [1536], P('tp'), may hold values from -3 to 3
- w_out: bfloat16 [1536, 2048], P('tp'), may hold values from -0.15625 to 0.15625
- gain_mix: float32 [2048], replicated, may hold values from 0.1 to 1.9
- w_group: bfloat16 [2048, 4], replicated, may hold values from -0.0625 to 0.0625
- w_expert: bfloat16 [2048, 64], replicated, may hold values from -0.0625 to 0.0625
- w_gate: bfloat16 [64, 2048, 1024], P('ep', None, 'tp'), may hold values from -0.125 to 0.125
- w_up: bfloat16 [64, 2048, 1024], P('ep', None, 'tp'), may hold values from -0.125 to 0.125
- w_down: bfloat16 [64, 1024, 2048], P('ep', 'tp'), may hold values from -3 to 3
- gain_moe: float32 [2048], replicated, may hold values from 0.1 to 1.9
Outputs:
- layer_out: bfloat16 [4096, 2048], P(('grp', 'ep')), parts along dimension 0
- new_state: float32 [4096, 96, 128], P(('grp', 'ep'), 'tp'), parts along dimension 0
The draws below stay inside these ranges and needn't reach their ends.
There are 2 independent parts, one for each index of `grp`. The reference program is written for one: setup_inputs(seed, part) draws one part's arguments, and reference() takes and returns one part's arrays. A program takes and returns all parts, laid end to end along the dimension named above; an argument that names none is the same for every part. Nothing has to cross between parts.
Inputs may be any that keep to these rules, and one draw needn't show every extreme that they name: `routes`: each row names two different experts of one group of 16 consecutive expert numbers. Within the rows of one index of ep (aligned blocks of 64 rows) no expert is named by more than 4 rows, and in every block some expert is named by exactly 4 rows.
All inputs are finite; a program needn't handle non-finite values.
Results may differ from the reference program's by a relative error of at most 0.015.
Values may be sent and summed in bfloat16 or wider, within the bound.
A program may use at most 64 MiB of HBM per device.

```python
import math
import jax
import jax.numpy as jnp
from jax import lax

D = 2048
MIX = 1536
GROUP = 16
CHGROUPS = 96
STATE = 64
MIX_DEV = 384
FF = 1024
FF_DEV = 256
TOP = 2
EXPERTS = 64
EGROUPS = 4
SEQ_DEV = 64
SEQS = 2048
CAP = 4
N_EP = 32
N_TP = 4


def shuffle_rows(key_row):
    return jax.random.permutation(key_row, SEQ_DEV).astype(jnp.int32)


def shuffle_group(key_group):
    return jax.random.permutation(key_group, EXPERTS // EGROUPS).astype(jnp.int32)


def draw_routes(key, part):
    block_count = SEQS // SEQ_DEV
    pair_count = EXPERTS // 2
    group_size = EXPERTS // EGROUPS
    key_pair, key_order, key_offset, key_rows = jax.random.split(key, 4)
    within = jax.vmap(shuffle_group)(jax.random.split(key_pair, EGROUPS))
    members = within + group_size * jnp.arange(EGROUPS, dtype=jnp.int32)[:, None]
    pair_table = members.reshape(pair_count, 2)
    pair_order = jax.random.permutation(key_order, pair_count).astype(jnp.int32)
    offsets = jax.random.randint(key_offset, (block_count, 1), 0, pair_count - 1).astype(jnp.int32)
    ranks = jnp.arange(SEQ_DEV, dtype=jnp.int32)[None, :]
    slot_pick = jnp.where(ranks < CAP, 0, 1 + (ranks - CAP + offsets) % (pair_count - 1))
    slot_pick = jnp.broadcast_to(slot_pick, (block_count, SEQ_DEV))
    shuffled = jax.vmap(shuffle_rows)(jax.random.split(key_rows, block_count))
    mixed_pick = jnp.take_along_axis(slot_pick, shuffled, axis=1)
    picked = pair_table[pair_order[mixed_pick]]
    return picked.reshape(SEQS, 2).astype(jnp.int32)


def steps_of(key, shape, cuts, smallest, top_value):
    loudness, own = 1.0, jax.random.fold_in(key, 6)
    for axis_at, shards_of in cuts:
        steps = jnp.exp(jax.random.uniform(jax.random.fold_in(own, axis_at), (shards_of,), jnp.float32, smallest / len(cuts), top_value / len(cuts)))
        loudness = loudness * jnp.repeat(steps, shape[axis_at] // shards_of).reshape([-1 if axis == axis_at else 1 for axis in range(len(shape))])
    return loudness


def noise(stream_key, dims, scale, bound, shards=(), held_as=jnp.bfloat16):
    result = jax.random.normal(stream_key, dims, jnp.float32) * scale
    if len(shards) > 0:
        result = steps_of(stream_key, dims, shards, -0.22, 0.18) * result
    return jnp.clip(result, min=-bound, max=bound).astype(held_as)


def setup_inputs(seed: int = 0, part: int = 0) -> dict:
    seeds = jax.random.split(jax.random.key(seed), 19)
    part_splits = jax.random.split(jax.random.fold_in(seeds[18], part), 19)
    return {
        "x_in": noise(part_splits[0], (SEQS, D), 1.0, 6.0, ((0, 32),)),
        "state": noise(part_splits[1], (SEQS, CHGROUPS, 2 * STATE), 1.0, 6.0, ((0, 32), (1, 4)), jnp.float32),
        "routes": draw_routes(jax.random.fold_in(jax.random.fold_in(seeds[18], part), 71), part),
        "w_in": noise(seeds[3], (D, MIX), D ** -0.5, 0.125, ((1, 4),)),
        "decay_rate": jnp.clip(jnp.exp(math.log(1.0) - 4.6051702 * jax.random.uniform(seeds[4], (CHGROUPS, STATE), jnp.float32) ** steps_of(seeds[4], (CHGROUPS, STATE), ((0, 4),), -0.2, 0.2)), 0.01, 1.0),
        "frequency": jnp.clip(192.0 * jax.random.uniform(seeds[5], (CHGROUPS, STATE), jnp.float32) ** steps_of(seeds[5], (CHGROUPS, STATE), ((0, 4),), -0.2, 0.2), 0.0, 192.0),
        "log_step": jnp.clip(-3.0 + 3.0 * jax.random.uniform(seeds[6], (CHGROUPS,), jnp.float32) ** steps_of(seeds[6], (CHGROUPS,), ((0, 4),), -0.2, 0.2), -3.0, 0.0),
        "b_in": noise(seeds[7], (CHGROUPS, GROUP, 2 * STATE), GROUP ** -0.5, 1.5, ((0, 4),), jnp.float32),
        "c_out": noise(seeds[8], (CHGROUPS, GROUP, 2 * STATE), (2 * STATE) ** -0.5, 0.5, ((0, 4),), jnp.float32),
        "skip": noise(seeds[9], (MIX,), 0.5, 3.0, ((0, 4),), jnp.float32),
        "w_out": noise(seeds[10], (MIX, D), MIX ** -0.5, 0.15625, ((0, 4),)),
        "gain_mix": jnp.clip(1.0 + 0.18 * jax.random.normal(seeds[11], (D,), jnp.float32), 0.1, 1.9),
        "w_group": noise(seeds[12], (D, EGROUPS), (4 * D) ** -0.5, 0.0625),
        "w_expert": noise(seeds[13], (D, EXPERTS), (4 * D) ** -0.5, 0.0625),
        "w_gate": noise(seeds[14], (EXPERTS, D, FF), D ** -0.5, 0.125, ((0, 32), (2, 4))),
        "w_up": noise(seeds[15], (EXPERTS, D, FF), D ** -0.5, 0.125, ((0, 32), (2, 4))),
        "w_down": noise(seeds[16], (EXPERTS, FF, D), (max(1, FF // 256)) ** -0.5, 3.0, ((0, 32), (1, 4))),
        "gain_moe": jnp.clip(1.0 + 0.18 * jax.random.normal(seeds[17], (D,), jnp.float32), 0.1, 1.9),
    }


residual_scale = 8.0 ** 0.25
norm_eps = 1e-05

def normalize(values, gain):
    centre = lax.optimization_barrier(jnp.mean(values, -1, keepdims=True))
    spread = lax.optimization_barrier(jnp.mean(jnp.square(values - centre), -1, keepdims=True))
    return (values - centre) * lax.rsqrt(spread + norm_eps) * gain

def s5_advance(mix_input, state, decay_rate, frequency, log_step, b_in, c_out, skip):
    top_precision = lax.Precision.HIGHEST
    entries = decay_rate.shape[-1]
    group_count = decay_rate.shape[0]
    width = b_in.shape[1]
    seq_count = mix_input.shape[0]
    input_rows = mix_input.astype(jnp.float32).reshape(seq_count, group_count, width)
    step_size = jnp.exp(log_step)[:, None]
    lam_real = -decay_rate
    lam_imag = frequency
    magnitude = jnp.exp(lam_real * step_size)
    angle_dt = lam_imag * step_size
    bar_real = magnitude * jnp.cos(angle_dt)
    bar_imag = magnitude * jnp.sin(angle_dt)
    minus_real = bar_real - 1.0
    modulus = lam_real * lam_real + lam_imag * lam_imag
    ratio_real = (minus_real * lam_real + bar_imag * lam_imag) / modulus
    ratio_imag = (bar_imag * lam_real - minus_real * lam_imag) / modulus
    in_real = b_in[..., :entries]
    in_imag = b_in[..., entries:]
    input_matrix_real = ratio_real[:, None, :] * in_real - ratio_imag[:, None, :] * in_imag
    input_matrix_imag = ratio_real[:, None, :] * in_imag + ratio_imag[:, None, :] * in_real
    forcing_real = jnp.einsum('rxf,xfb->rxb', input_rows, input_matrix_real, precision=top_precision)
    forcing_imag = jnp.einsum('rxf,xfb->rxb', input_rows, input_matrix_imag, precision=top_precision)
    old_real = state[..., :entries]
    old_imag = state[..., entries:]
    following_real = bar_real * old_real - bar_imag * old_imag + forcing_real
    following_imag = bar_real * old_imag + bar_imag * old_real + forcing_imag
    output_real = c_out[..., :entries]
    output_imag = c_out[..., entries:]
    output_matrix = jnp.einsum('lzt,zft->lzf', following_real, output_real, precision=top_precision)
    output_matrix = output_matrix - jnp.einsum('lzt,zft->lzf', following_imag, output_imag, precision=top_precision)
    output_matrix = output_matrix + skip.reshape(group_count, width) * input_rows
    activated = jax.nn.gelu(output_matrix).reshape(seq_count, group_count * width)
    return (activated, jnp.concatenate([following_real, following_imag], axis=-1))

def route_weights(normed, routes, w_group, w_expert):
    group_total = w_group.shape[1]
    expert_total = w_expert.shape[1]
    per_group = expert_total // group_total
    group_logit = jnp.dot(normed, w_group, preferred_element_type=jnp.float32)
    group_exp = jnp.exp(group_logit)
    group_prob = group_exp / lax.optimization_barrier(jnp.sum(group_exp, -1, keepdims=True))
    chosen = routes[:, 0] // per_group
    group_pick = lax.optimization_barrier(jnp.sum(jnp.where(chosen[:, None] == jnp.arange(group_total, dtype=jnp.int32)[None, :], group_prob, 0.0), -1))
    expert_logit = jnp.dot(normed, w_expert, preferred_element_type=jnp.float32)
    picked = lax.optimization_barrier(jnp.sum(jnp.where(routes[:, :, None] == jnp.arange(expert_total, dtype=jnp.int32)[None, None, :], expert_logit[:, None, :], 0.0), -1))
    pair_exp = jnp.exp(picked)
    return pair_exp / lax.optimization_barrier(jnp.sum(pair_exp, -1, keepdims=True)) * group_pick[:, None]

def reference(x_in, state, routes, w_in, decay_rate, frequency, log_step, b_in, c_out, skip, w_out, gain_mix, w_group, w_expert, w_gate, w_up, w_down, gain_moe):
    mix_input = jnp.dot(x_in, w_in, preferred_element_type=jnp.float32).astype(jnp.bfloat16)
    activated, new_state = s5_advance(mix_input, state, decay_rate, frequency, log_step, b_in, c_out, skip)
    mix_act = activated.astype(jnp.bfloat16)
    block_parts = jnp.einsum('ntc,tcd->ntd', mix_act.astype(jnp.float32).reshape(SEQS, N_TP, MIX_DEV), w_out.astype(jnp.float32).reshape(N_TP, MIX_DEV, D))
    block_parts = lax.optimization_barrier(block_parts.astype(jnp.bfloat16))
    mixed = lax.optimization_barrier(jnp.sum(block_parts.astype(jnp.float32), axis=1))
    hidden_state = normalize(residual_scale * x_in.astype(jnp.float32) + mixed, gain_mix)
    hidden_bf = hidden_state.astype(jnp.bfloat16)
    route_weight = route_weights(hidden_bf, routes, w_group, w_expert)
    block_routes = routes.reshape(N_EP, SEQ_DEV, TOP)
    hits = (block_routes[..., None] == jnp.arange(EXPERTS, dtype=jnp.int32)).astype(jnp.int32)
    tally = lax.optimization_barrier(jnp.sum(hits, axis=2))
    prior = jnp.cumsum(tally, axis=1) - tally
    slot_in_block = lax.optimization_barrier(jnp.sum(prior[:, :, None, :] * hits, axis=-1))
    block_index = jnp.arange(N_EP, dtype=jnp.int32)[:, None, None]
    position = (block_index * CAP + slot_in_block).reshape(-1).astype(jnp.int32)
    expert_flat = routes.reshape(-1).astype(jnp.int32)
    row_copies = jnp.broadcast_to(hidden_bf[:, None, :], (SEQS, TOP, D)).reshape(SEQS * TOP, D)
    buffer = jnp.zeros((EXPERTS, N_EP * CAP, D), jnp.bfloat16).at[expert_flat, position].set(row_copies)

    def one_expert(operands):
        slot_rows, gate_weight, up_weight, down_weight = operands
        gate_val = jnp.dot(slot_rows, gate_weight, preferred_element_type=jnp.float32)
        up_val = jnp.dot(slot_rows, up_weight, preferred_element_type=jnp.float32)
        act = (jax.nn.silu(gate_val) * up_val).astype(jnp.bfloat16)
        pieces = jnp.einsum('rtf,tfd->rtd', act.astype(jnp.float32).reshape(N_EP * CAP, N_TP, FF_DEV), down_weight.astype(jnp.float32).reshape(N_TP, FF_DEV, D))
        pieces = lax.optimization_barrier(pieces.astype(jnp.bfloat16))
        return lax.optimization_barrier(jnp.sum(pieces.astype(jnp.float32), axis=1)).astype(jnp.bfloat16)
    outputs = lax.map(one_expert, (buffer, w_gate, w_up, w_down))
    expert_out = outputs[expert_flat, position].reshape(SEQS, TOP, D).astype(jnp.float32)
    moe = lax.optimization_barrier(jnp.sum(route_weight[:, :, None] * expert_out, axis=1))
    layer_out = normalize(residual_scale * hidden_state + moe, gain_moe).astype(jnp.bfloat16)
    return (layer_out, new_state)
```

```python
import functools

import jax
import jax.numpy as jnp
from jax import lax
from jax.experimental import pallas as pl
from jax.experimental.pallas import tpu as pltpu
from jax.sharding import PartitionSpec as P

residual_scale = 8.0**0.25
norm_eps = 1e-05
CORES = 2
CHUNKS = 4
F32 = jnp.float32
BF16 = jnp.bfloat16
MESH = pl.DeviceIdType.MESH


def dot(a, b):
    return jnp.dot(a, b, preferred_element_type=F32)


def chip_offsets(chips):
    order = [0]
    for step in range(1, chips // 2):
        order += [step, chips - step]
    order.append(chips // 2)
    size = chips // CHUNKS
    return [order[k * size : (k + 1) * size] for k in range(CHUNKS)]


def layer_kernel(
    n_ep,
    n_tp,
    x_h,
    state_h,
    routes_h,
    win_h,
    decay_h,
    freq_h,
    lstep_h,
    b_h,
    c_h,
    skip_h,
    wout_h,
    gmix_h,
    wgrp_h,
    wexp_h,
    wg_h,
    wu_h,
    wd_h,
    gmoe_h,
    out_h,
    ns_h,
    x_v,
    state_v,
    routes_v,
    win_v,
    decay_v,
    freq_v,
    lstep_v,
    b_v,
    c_v,
    skip_v,
    wout_v,
    gmix_v,
    wgrp_v,
    wexp_v,
    wg_v,
    wu_v,
    wd_v,
    gmoe_v,
    ns_v,
    out_part,
    out_recv,
    hid_v,
    stat_send,
    stat_recv,
    z_buf,
    z_recv_buf,
    gather_buf,
    down_part,
    down_recv,
    ret_send,
    ret_buf,
    fin_v,
    load_sem,
    store_sem,
    a_send,
    a_recv,
    s_send,
    s_recv,
    z_send,
    z_recv,
    x_send,
    x_recv,
    d_send,
    d_recv,
    r_send,
    r_recv,
    f_send,
    f_recv,
):
    ep = lax.axis_index("ep")
    tp = lax.axis_index("tp")
    chips = n_ep // CORES
    chip = ep // CORES
    core = ep % CORES
    rows, width = x_v.shape
    share = width // n_tp
    entries = decay_v.shape[1]
    lanes = 2 * entries
    groups = decay_v.shape[0]
    group_width = b_v.shape[0] // groups
    experts = wexp_v.shape[1]
    egroups = wgrp_v.shape[1]
    local_experts = wg_v.shape[0]
    cap = z_buf.shape[1] // local_experts
    slots = z_buf.shape[1]
    offsets = chip_offsets(chips)
    per_chunk = n_ep // CHUNKS
    chunk_rows = per_chunk * slots
    share_at = pl.ds(pl.multiple_of(tp * share, share), share)

    barrier = pltpu.get_barrier_semaphore()

    def greet_ep(i, _):
        peer = (ep + i) % n_ep
        pl.semaphore_signal(barrier, inc=1, device_id={"ep": peer}, device_id_type=MESH)
        return 0

    for r in range(1, n_tp):
        pl.semaphore_signal(
            barrier, inc=1, device_id={"tp": (tp + r) % n_tp}, device_id_type=MESH
        )
    lax.fori_loop(1, n_ep, greet_ep, 0)

    loads = {}
    pairs = (
        ("x", x_h, x_v),
        ("win", win_h, win_v),
        ("decay", decay_h, decay_v),
        ("freq", freq_h, freq_v),
        ("lstep", lstep_h, lstep_v),
        ("b", b_h, b_v),
        ("c", c_h, c_v),
        ("state", state_h, state_v),
        ("skip", skip_h, skip_v),
        ("wout", wout_h, wout_v),
        ("gmix", gmix_h.at[:, share_at], gmix_v),
        ("routes", routes_h, routes_v),
        ("wgrp", wgrp_h.at[share_at, :], wgrp_v),
        ("wexp", wexp_h.at[share_at, :], wexp_v),
        ("wg", wg_h, wg_v),
        ("wu", wu_h, wu_v),
        ("wd", wd_h, wd_v),
        ("gmoe", gmoe_h.at[:, share_at], gmoe_v),
    )
    for i, (name, src, dst) in enumerate(pairs):
        loads[name] = pltpu.make_async_copy(src, dst, load_sem.at[i])
        loads[name].start()

    sends = []

    def send(src, dst, send_sem, recv_sem, target):
        copy = pltpu.make_async_remote_copy(
            src_ref=src,
            dst_ref=dst,
            send_sem=send_sem,
            recv_sem=recv_sem,
            device_id=target,
            device_id_type=MESH,
        )
        copy.start()
        sends.append(copy)
        return copy

    for name in ("decay", "freq", "lstep", "b", "c"):
        loads[name].wait()
    eye = (
        lax.broadcasted_iota(jnp.int32, (groups, groups), 0)
        == lax.broadcasted_iota(jnp.int32, (groups, groups), 1)
    )
    log_step = jnp.sum(jnp.where(eye, lstep_v[...], 0.0), axis=1, keepdims=True)
    step_size = jnp.exp(log_step)
    decay = decay_v[...]
    freq = freq_v[...]
    lam_real = -decay
    magnitude = jnp.exp(lam_real * step_size)
    angle = freq * step_size
    bar_real = magnitude * jnp.cos(angle)
    bar_imag = magnitude * jnp.sin(angle)
    minus_real = bar_real - 1.0
    modulus = lam_real * lam_real + freq * freq
    ratio_real = (minus_real * lam_real + bar_imag * freq) / modulus
    ratio_imag = (bar_imag * lam_real - minus_real * freq) / modulus
    bar_same = jnp.concatenate([bar_real, bar_real], axis=1)
    bar_cross = jnp.concatenate([-bar_imag, bar_imag], axis=1)
    ratio_same = jnp.concatenate([ratio_real, ratio_real], axis=1)
    ratio_cross = jnp.concatenate([-ratio_imag, ratio_imag], axis=1)

    loads["x"].wait()
    loads["win"].wait()
    mix_input = dot(x_v[...], win_v[...]).astype(BF16)
    loads["skip"].wait()
    loads["state"].wait()

    per_block = lanes // group_width
    block_lanes = per_block * lanes
    own_group = (
        lax.broadcasted_iota(jnp.int32, (lanes, block_lanes), 0) // group_width
        == lax.broadcasted_iota(jnp.int32, (lanes, block_lanes), 1) // lanes
    )
    sign = jnp.where(lax.broadcasted_iota(jnp.int32, (1, lanes), 1) < entries, 1.0, -1.0)
    acts = []
    for j in range(groups // per_block):
        channels = slice(j * lanes, (j + 1) * lanes)
        bars = []
        for g in range(j * per_block, (j + 1) * per_block):
            b_g = b_v[g * group_width : (g + 1) * group_width, :]
            bars.append(
                b_g * ratio_same[g : g + 1, :]
                + pltpu.roll(b_g, entries, 1) * ratio_cross[g : g + 1, :]
            )
        b_bar = jnp.concatenate(bars, axis=0)
        b_wide = jnp.where(own_group, jnp.concatenate([b_bar] * per_block, axis=1), 0.0)
        u_j = mix_input[:, channels]
        forcing = dot(u_j, b_wide.astype(BF16))
        news = []
        for i in range(per_block):
            g = j * per_block + i
            old = state_v[pl.ds(g, rows, stride=groups), :]
            new = (
                old * bar_same[g : g + 1, :]
                + pltpu.roll(old, entries, 1) * bar_cross[g : g + 1, :]
                + forcing[:, i * lanes : (i + 1) * lanes]
            )
            ns_v[pl.ds(g, rows, stride=groups), :] = new
            news.append(new.astype(BF16))
        c_j = c_v[channels, :] * sign
        c_wide = jnp.where(own_group, jnp.concatenate([c_j] * per_block, axis=1), 0.0)
        y = lax.dot_general(
            jnp.concatenate(news, axis=1),
            c_wide.astype(BF16),
            (((1,), (1,)), ((), ())),
            preferred_element_type=F32,
        )
        y = y + skip_v[:, channels] * u_j.astype(F32)
        acts.append(jax.nn.gelu(y).astype(BF16))
    store = pltpu.make_async_copy(ns_v, ns_h, store_sem)
    store.start()
    act_mix = jnp.concatenate(acts, axis=1)

    loads["wout"].wait()
    pl.semaphore_wait(barrier, n_ep - 1 + n_tp - 1)
    waits = {}
    for r in (2, 1, 3, 0):
        q = (tp + r) % n_tp
        cols = pl.ds(pl.multiple_of(q * share, share), share)
        out_part[r] = dot(act_mix, wout_v[:, cols]).astype(BF16)
        if r:
            waits[r] = send(
                out_part.at[r], out_recv.at[r - 1], a_send.at[r - 1], a_recv.at[r - 1], {"tp": q}
            )

    for name in ("routes", "gmix", "wgrp", "wexp"):
        loads[name].wait()
    route = [routes_v[:, k : k + 1] for k in range(2)]
    expert_id = lax.broadcasted_iota(jnp.int32, (rows, experts), 1)
    chosen = [(route[k] == expert_id).astype(F32) for k in range(2)]
    hits = chosen[0] + chosen[1]
    row_id = lax.broadcasted_iota(jnp.int32, (rows, rows), 0)
    col_id = lax.broadcasted_iota(jnp.int32, (rows, rows), 1)
    earlier = (row_id > col_id).astype(BF16)
    prior = dot(earlier, hits.astype(BF16))
    slot_id = lax.broadcasted_iota(jnp.int32, (rows, experts * cap), 1).astype(F32)
    places = []
    for k in range(2):
        rank = jnp.sum(prior * chosen[k], axis=1, keepdims=True)
        target = route[k].astype(F32) * cap + rank
        places.append((target == slot_id).astype(F32))
    dispatch_map = (places[0] + places[1]).astype(BF16)

    diagonal = (
        lax.broadcasted_iota(jnp.int32, (rows, 128), 0)
        == lax.broadcasted_iota(jnp.int32, (rows, 128), 1)
    )

    def exchange(n, columns):
        for i, column in enumerate(columns):
            stat_send[n, i : i + 1, :] = jnp.sum(
                jnp.where(diagonal, column, 0.0), axis=0, keepdims=True
            )
        for r in (2, 1, 3):
            send(
                stat_send.at[n],
                stat_recv.at[n, r - 1],
                s_send.at[n, r - 1],
                s_recv.at[n, r - 1],
                {"tp": (tp + r) % n_tp},
            )

    def received(n, count):
        for r in range(1, n_tp):
            pltpu.make_async_copy(
                stat_recv.at[n, r - 1], stat_recv.at[n, r - 1], s_recv.at[n, r - 1]
            ).wait()
        parts = [stat_send[n]] + [stat_recv[n, r - 1] for r in range(1, n_tp)]
        return [
            [
                jnp.sum(jnp.where(diagonal, part[i : i + 1, :], 0.0), axis=1, keepdims=True)
                for i in range(count)
            ]
            for part in parts
        ]

    def norm_terms(n, values):
        mean_own = jnp.mean(values, axis=1, keepdims=True)
        spread_own = jnp.sum(jnp.square(values - mean_own), axis=1, keepdims=True)
        exchange(n, [mean_own, spread_own])
        stats = received(n, 2)
        mean = sum(s[0] for s in stats) / n_tp
        spread = sum(s[1] + share * jnp.square(s[0] - mean) for s in stats) / width
        return mean, lax.rsqrt(spread + norm_eps)

    for r in range(1, n_tp):
        waits[r].wait_recv()
    mixed = out_part[0].astype(F32)
    for r in range(1, n_tp):
        mixed = mixed + out_recv[r - 1].astype(F32)
    values = residual_scale * x_v[:, share_at].astype(F32) + mixed
    mean, scale = norm_terms(0, values)
    hidden = (values - mean) * scale * gmix_v[...]
    hid_v[...] = hidden
    hidden_bf = hidden.astype(BF16)

    z_buf[...] = (
        lax.dot_general(
            dispatch_map, hidden_bf, (((0,), (0,)), ((), ())), preferred_element_type=F32
        )
        .reshape(n_ep, slots, share)
        .astype(BF16)
    )
    z_recv_buf[0, core] = z_buf[ep]
    for k in range(CHUNKS):
        for i, offset in enumerate(offsets[k]):
            for c in (1, 0):
                if offset == 0 and c == 0:
                    continue
                target = ((chip + chips - offset) % chips) * CORES + (core + c) % CORES
                send(
                    z_buf.at[target],
                    z_recv_buf.at[k, i * CORES + core],
                    z_send.at[(k * len(offsets[k]) + i) * CORES + c],
                    z_recv.at[k],
                    {"ep": target},
                )

    group_logit = dot(hidden_bf, wgrp_v[...])
    expert_logit = dot(hidden_bf, wexp_v[...])
    columns = [jnp.sum(chosen[k] * expert_logit, axis=1, keepdims=True) for k in range(2)]
    columns += [group_logit[:, i : i + 1] for i in range(egroups)]
    exchange(1, columns)

    def wait_bytes(ref, sem):
        pltpu.make_async_copy(ref, ref, sem).wait()

    def gather(k):
        count = per_chunk - 1 if k == 0 else per_chunk
        wait_bytes(z_recv_buf.at[k, 0:count], z_recv.at[k])
        for r in (2, 1, 3):
            send(
                z_recv_buf.at[k],
                gather_buf.at[k, tp],
                x_send.at[k, r - 1],
                x_recv.at[k, r - 1],
                {"tp": (tp + r) % n_tp},
            )
        gather_buf[k, tp] = z_recv_buf[k]

    def experts_of(k):
        for r in range(1, n_tp):
            wait_bytes(gather_buf.at[k, 0], x_recv.at[k, r - 1])
        if k == 0:
            for name in ("wg", "wu", "wd"):
                loads[name].wait()
        lhs = [gather_buf[k, t].reshape(chunk_rows, share) for t in range(n_tp)]
        lhs = jnp.concatenate(lhs, axis=1)
        slot = lax.broadcasted_iota(jnp.int32, (chunk_rows, 1), 0) % slots
        acts = []
        for e in range(local_experts):
            gate = dot(lhs, wg_v[e])
            up = dot(lhs, wu_v[e])
            mine = slot // cap == e
            acts.append(jnp.where(mine, jax.nn.silu(gate) * up, 0.0).astype(BF16))
        act = jnp.concatenate(acts, axis=1)
        for r in (2, 1, 3, 0):
            q = (tp + r) % n_tp
            cols = pl.ds(pl.multiple_of(q * share, share), share)
            down_part[k, r] = dot(act, wd_v[:, cols]).astype(BF16)
            if r:
                send(
                    down_part.at[k, r],
                    down_recv.at[k, r - 1],
                    d_send.at[k, r - 1],
                    d_recv.at[k, r - 1],
                    {"tp": q},
                )

    def give_back(k):
        for r in range(1, n_tp):
            wait_bytes(down_recv.at[k, r - 1], d_recv.at[k, r - 1])
        total = down_part[k, 0].astype(F32)
        for r in range(1, n_tp):
            total = total + down_recv[k, r - 1].astype(F32)
        ret_send[k] = total.reshape(per_chunk, slots, share).astype(BF16)
        for i, offset in enumerate(offsets[k]):
            for c in (1, 0):
                to_core = (core + c) % CORES
                if offset == 0 and c == 0:
                    continue
                target = ((chip + offset) % chips) * CORES + to_core
                send(
                    ret_send.at[k, i * CORES + to_core],
                    ret_buf.at[ep],
                    r_send.at[(k * len(offsets[k]) + i) * CORES + c],
                    r_recv,
                    {"ep": target},
                )
        if k == 0:
            ret_buf[ep] = ret_send[0, core]

    gather(0)
    gather(1)
    experts_of(0)
    for k in range(2, CHUNKS):
        gather(k)
        experts_of(k - 1)
        give_back(k - 2)
    experts_of(CHUNKS - 1)
    give_back(CHUNKS - 2)

    parts = received(1, 2 + egroups)
    total = [sum(p[i] for p in parts) for i in range(2 + egroups)]
    pair = [jnp.exp(total[k]) for k in range(2)]
    group_exp = [jnp.exp(total[2 + i]) for i in range(egroups)]
    own = route[0] // (experts // egroups)
    picked = sum(jnp.where(own == i, group_exp[i], 0.0) for i in range(egroups))
    group_prob = picked / sum(group_exp)
    pair_sum = pair[0] + pair[1]
    combine_map = sum(places[k] * (pair[k] / pair_sum * group_prob) for k in range(2))
    combine_map = combine_map.astype(BF16)
    loads["gmoe"].wait()

    give_back(CHUNKS - 1)

    wait_bytes(ret_buf.at[0 : n_ep - 1], r_recv)
    returned = ret_buf[...].reshape(n_ep * slots, share)
    values = residual_scale * hid_v[...] + dot(combine_map, returned)
    mean, scale = norm_terms(2, values)
    fin_v[...] = ((values - mean) * scale * gmoe_v[...]).astype(BF16)
    last = []
    for r in (2, 1, 3):
        last.append(
            send(
                fin_v,
                out_h.at[:, share_at],
                f_send.at[r - 1],
                f_recv.at[r - 1],
                {"tp": (tp + r) % n_tp},
            )
        )
    own_store = pltpu.make_async_copy(fin_v, out_h.at[:, share_at], f_send.at[n_tp - 1])
    own_store.start()
    for copy in last:
        copy.wait_recv()
    own_store.wait()
    store.wait()
    for copy in sends:
        copy.wait_send()


def per_device(
    n_ep,
    n_tp,
    x_in,
    state,
    routes,
    w_in,
    decay_rate,
    frequency,
    log_step,
    b_in,
    c_out,
    skip,
    w_out,
    gain_mix,
    w_group,
    w_expert,
    w_gate,
    w_up,
    w_down,
    gain_moe,
):
    rows, width = x_in.shape
    share = width // n_tp
    groups, entries = decay_rate.shape
    lanes = 2 * entries
    channels = skip.shape[0]
    experts = w_expert.shape[1]
    egroups = w_group.shape[1]
    local_experts, _, hidden_units = w_gate.shape
    cap = max(2, 4 * rows // experts)
    slots = local_experts * cap
    per_chunk = n_ep // CHUNKS
    args = (
        x_in,
        state.reshape(rows * groups, lanes),
        routes,
        w_in,
        decay_rate,
        frequency,
        log_step.reshape(1, groups),
        b_in.reshape(channels, lanes),
        c_out.reshape(channels, lanes),
        skip.reshape(1, channels),
        w_out,
        gain_mix.reshape(1, width),
        w_group,
        w_expert,
        w_gate,
        w_up,
        w_down.reshape(local_experts * hidden_units, width),
        gain_moe.reshape(1, width),
    )
    dma = pltpu.SemaphoreType.DMA
    peers = n_tp - 1
    scratch = [
        pltpu.VMEM((rows, width), BF16),
        pltpu.VMEM((rows * groups, lanes), F32),
        pltpu.VMEM(routes.shape, jnp.int32),
        pltpu.VMEM(w_in.shape, BF16),
        pltpu.VMEM(decay_rate.shape, F32),
        pltpu.VMEM(frequency.shape, F32),
        pltpu.VMEM((1, groups), F32),
        pltpu.VMEM((channels, lanes), F32),
        pltpu.VMEM((channels, lanes), F32),
        pltpu.VMEM((1, channels), F32),
        pltpu.VMEM(w_out.shape, BF16),
        pltpu.VMEM((1, share), F32),
        pltpu.VMEM((share, egroups), BF16),
        pltpu.VMEM((share, experts), BF16),
        pltpu.VMEM(w_gate.shape, BF16),
        pltpu.VMEM(w_up.shape, BF16),
        pltpu.VMEM((local_experts * hidden_units, width), BF16),
        pltpu.VMEM((1, share), F32),
        pltpu.VMEM((rows * groups, lanes), F32),
        pltpu.VMEM((n_tp, rows, share), BF16),
        pltpu.VMEM((peers, rows, share), BF16),
        pltpu.VMEM((rows, share), F32),
        pltpu.VMEM((3, 8, 128), F32),
        pltpu.VMEM((3, peers, 8, 128), F32),
        pltpu.VMEM((n_ep, slots, share), BF16),
        pltpu.VMEM((CHUNKS, per_chunk, slots, share), BF16),
        pltpu.VMEM((CHUNKS, n_tp, per_chunk, slots, share), BF16),
        pltpu.VMEM((CHUNKS, n_tp, per_chunk * slots, share), BF16),
        pltpu.VMEM((CHUNKS, peers, per_chunk * slots, share), BF16),
        pltpu.VMEM((CHUNKS, per_chunk, slots, share), BF16),
        pltpu.VMEM((n_ep, slots, share), BF16),
        pltpu.VMEM((rows, share), BF16),
        dma((len(args),)),
        dma,
        dma((peers,)),
        dma((peers,)),
        dma((3, peers)),
        dma((3, peers)),
        dma((n_ep,)),
        dma((CHUNKS,)),
        dma((CHUNKS, peers)),
        dma((CHUNKS, peers)),
        dma((CHUNKS, peers)),
        dma((CHUNKS, peers)),
        dma((n_ep,)),
        dma,
        dma((n_tp,)),
        dma((peers,)),
    ]
    any_space = pl.BlockSpec(memory_space=pl.ANY)
    out, new_state = pl.pallas_call(
        functools.partial(layer_kernel, n_ep, n_tp),
        out_shape=(
            jax.ShapeDtypeStruct((rows, width), BF16),
            jax.ShapeDtypeStruct((rows * groups, lanes), F32),
        ),
        in_specs=[any_space] * len(args),
        out_specs=(any_space, any_space),
        scratch_shapes=scratch,
        compiler_params=pltpu.CompilerParams(
            collective_id=0, has_side_effects=True, vmem_limit_bytes=60 * 1024 * 1024
        ),
        name="layer",
    )(*args)
    return out, new_state.reshape(state.shape)


def solution(mesh):
    in_specs = (
        P(("grp", "ep"), None),
        P(("grp", "ep"), "tp", None),
        P(("grp", "ep"), None),
        P(None, "tp"),
        P("tp", None),
        P("tp", None),
        P("tp"),
        P("tp", None, None),
        P("tp", None, None),
        P("tp"),
        P("tp", None),
        P(),
        P(),
        P(),
        P("ep", None, "tp"),
        P("ep", None, "tp"),
        P("ep", "tp", None),
        P(),
    )
    out_specs = (P(("grp", "ep"), None), P(("grp", "ep"), "tp", None))
    return jax.shard_map(
        functools.partial(per_device, mesh.shape["ep"], mesh.shape["tp"]),
        mesh=mesh,
        in_specs=in_specs,
        out_specs=out_specs,
        check_vma=False,
    )
```

```python
import functools

import jax
import jax.numpy as jnp
from jax import lax
from jax.experimental import pallas as pl
from jax.experimental.pallas import tpu as pltpu
from jax.sharding import PartitionSpec as P

residual_scale = 8.0**0.25
norm_eps = 1e-05
CORES = 2
CHUNKS = 4
F32 = jnp.float32
BF16 = jnp.bfloat16
MESH = pl.DeviceIdType.MESH


def dot(a, b):
    return jnp.dot(a, b, preferred_element_type=F32)


def dot_t(a, b):
    return lax.dot_general(a, b, (((1,), (1,)), ((), ())), preferred_element_type=F32)


def chip_offsets(chips):
    order = [0]
    for step in range(1, chips // 2):
        order += [step, chips - step]
    order.append(chips // 2)
    size = chips // CHUNKS
    return [order[k * size : (k + 1) * size] for k in range(CHUNKS)]


def layer_kernel(
    n_ep,
    n_tp,
    x_h,
    state_h,
    routes_h,
    win_h,
    decay_h,
    freq_h,
    lstep_h,
    b_h,
    c_h,
    skip_h,
    wout_h,
    gmix_h,
    wgrp_h,
    wexp_h,
    wg_h,
    wu_h,
    wd_h,
    gmoe_h,
    out_h,
    ns_h,
    x_v,
    state_v,
    routes_v,
    win_v,
    decay_v,
    freq_v,
    lstep_v,
    b_v,
    c_v,
    skip_v,
    wout_v,
    gmix_v,
    wgrp_v,
    wexp_v,
    wg_v,
    wu_v,
    wd_v,
    gmoe_v,
    ns_v,
    out_part,
    out_recv,
    hid_v,
    stat_send,
    stat_recv,
    z_buf,
    z_recv_buf,
    gather_buf,
    down_part,
    down_recv,
    ret_send,
    ret_buf,
    fin_v,
    load_sem,
    store_sem,
    a_send,
    a_recv,
    s_send,
    s_recv,
    z_send,
    z_recv,
    x_send,
    x_recv,
    d_send,
    d_recv,
    r_send,
    r_recv,
    f_send,
    f_recv,
):
    ep = lax.axis_index("ep")
    tp = lax.axis_index("tp")
    chips = n_ep // CORES
    chip = ep // CORES
    core = ep % CORES
    rows, width = x_v.shape
    share = width // n_tp
    entries = decay_v.shape[1]
    lanes = 2 * entries
    groups = decay_v.shape[0]
    group_width = b_v.shape[0] // groups
    experts = wexp_v.shape[0]
    egroups = wgrp_v.shape[0]
    local_experts = wg_v.shape[0]
    cap = z_buf.shape[1] // local_experts
    slots = z_buf.shape[1]
    offsets = chip_offsets(chips)
    per_chunk = n_ep // CHUNKS
    chunk_rows = per_chunk * slots
    share_at = pl.ds(pl.multiple_of(tp * share, share), share)

    barrier = pltpu.get_barrier_semaphore()

    def greet_ep(i, _):
        peer = (ep + i) % n_ep
        pl.semaphore_signal(barrier, inc=1, device_id={"ep": peer}, device_id_type=MESH)
        return 0

    for r in range(1, n_tp):
        pl.semaphore_signal(
            barrier, inc=1, device_id={"tp": (tp + r) % n_tp}, device_id_type=MESH
        )
    lax.fori_loop(1, n_ep, greet_ep, 0)

    loads = {}
    pairs = (
        ("x", x_h, x_v),
        ("win", win_h, win_v),
        ("decay", decay_h, decay_v),
        ("freq", freq_h, freq_v),
        ("lstep", lstep_h, lstep_v),
        ("b", b_h, b_v),
        ("c", c_h, c_v),
        ("state", state_h, state_v),
        ("skip", skip_h, skip_v),
        ("wout", wout_h, wout_v),
        ("gmix", gmix_h.at[:, share_at], gmix_v),
        ("routes", routes_h, routes_v),
        ("wgrp", wgrp_h.at[:, share_at], wgrp_v),
        ("wexp", wexp_h.at[:, share_at], wexp_v),
        ("wg", wg_h, wg_v),
        ("wu", wu_h, wu_v),
        ("wd", wd_h, wd_v),
        ("gmoe", gmoe_h.at[:, share_at], gmoe_v),
    )
    for i, (name, src, dst) in enumerate(pairs):
        loads[name] = pltpu.make_async_copy(src, dst, load_sem.at[i])
        loads[name].start()

    sends = []

    def send(src, dst, send_sem, recv_sem, target):
        copy = pltpu.make_async_remote_copy(
            src_ref=src,
            dst_ref=dst,
            send_sem=send_sem,
            recv_sem=recv_sem,
            device_id=target,
            device_id_type=MESH,
        )
        copy.start()
        sends.append(copy)
        return copy

    for name in ("decay", "freq", "lstep", "b", "c"):
        loads[name].wait()
    eye = (
        lax.broadcasted_iota(jnp.int32, (groups, groups), 0)
        == lax.broadcasted_iota(jnp.int32, (groups, groups), 1)
    )
    log_step = jnp.sum(jnp.where(eye, lstep_v[...], 0.0), axis=1, keepdims=True)
    step_size = jnp.exp(log_step)
    decay = decay_v[...]
    freq = freq_v[...]
    lam_real = -decay
    magnitude = jnp.exp(lam_real * step_size)
    angle = freq * step_size
    bar_real = magnitude * jnp.cos(angle)
    bar_imag = magnitude * jnp.sin(angle)
    minus_real = bar_real - 1.0
    modulus = lam_real * lam_real + freq * freq
    ratio_real = (minus_real * lam_real + bar_imag * freq) / modulus
    ratio_imag = (bar_imag * lam_real - minus_real * freq) / modulus
    bar_same = jnp.concatenate([bar_real, bar_real], axis=1)
    bar_cross = jnp.concatenate([-bar_imag, bar_imag], axis=1)
    ratio_same = jnp.concatenate([ratio_real, ratio_real], axis=1)
    ratio_cross = jnp.concatenate([-ratio_imag, ratio_imag], axis=1)

    loads["x"].wait()
    loads["win"].wait()
    mix_input = dot(x_v[...], win_v[...]).astype(BF16)
    loads["skip"].wait()
    loads["state"].wait()

    per_block = lanes // group_width
    block_lanes = per_block * lanes
    own_group = (
        lax.broadcasted_iota(jnp.int32, (lanes, block_lanes), 0) // group_width
        == lax.broadcasted_iota(jnp.int32, (lanes, block_lanes), 1) // lanes
    )
    sign = jnp.where(lax.broadcasted_iota(jnp.int32, (1, lanes), 1) < entries, 1.0, -1.0)
    acts = []
    for j in range(groups // per_block):
        channels = slice(j * lanes, (j + 1) * lanes)
        bars = []
        for g in range(j * per_block, (j + 1) * per_block):
            b_g = b_v[g * group_width : (g + 1) * group_width, :]
            bars.append(
                b_g * ratio_same[g : g + 1, :]
                + pltpu.roll(b_g, entries, 1) * ratio_cross[g : g + 1, :]
            )
        b_bar = jnp.concatenate(bars, axis=0)
        b_wide = jnp.where(own_group, jnp.concatenate([b_bar] * per_block, axis=1), 0.0)
        u_j = mix_input[:, channels]
        forcing = dot(u_j, b_wide.astype(BF16))
        news = []
        for i in range(per_block):
            g = j * per_block + i
            old = state_v[pl.ds(g, rows, stride=groups), :]
            new = (
                old * bar_same[g : g + 1, :]
                + pltpu.roll(old, entries, 1) * bar_cross[g : g + 1, :]
                + forcing[:, i * lanes : (i + 1) * lanes]
            )
            ns_v[pl.ds(g, rows, stride=groups), :] = new
            news.append(new.astype(BF16))
        c_j = c_v[channels, :] * sign
        c_wide = jnp.where(own_group, jnp.concatenate([c_j] * per_block, axis=1), 0.0)
        y = dot_t(jnp.concatenate(news, axis=1), c_wide.astype(BF16))
        y = y + skip_v[j : j + 1, :] * u_j.astype(F32)
        acts.append(jax.nn.gelu(y).astype(BF16))
    store = pltpu.make_async_copy(ns_v, ns_h, store_sem)
    store.start()
    act_mix = jnp.concatenate(acts, axis=1)

    loads["wout"].wait()
    pl.semaphore_wait(barrier, n_ep - 1 + n_tp - 1)
    waits = {}
    for r in (2, 1, 3, 0):
        q = (tp + r) % n_tp
        cols = pl.ds(pl.multiple_of(q * share, share), share)
        out_part[r] = dot(act_mix, wout_v[:, cols]).astype(BF16)
        if r:
            waits[r] = send(
                out_part.at[r], out_recv.at[r - 1], a_send.at[r - 1], a_recv.at[r - 1], {"tp": q}
            )

    for name in ("routes", "gmix", "wgrp", "wexp"):
        loads[name].wait()
    route = [
        jnp.sum(
            jnp.where(
                lax.broadcasted_iota(jnp.int32, (rows, rows), 0)
                == lax.broadcasted_iota(jnp.int32, (rows, rows), 1),
                routes_v[k : k + 1, :].astype(F32),
                0.0,
            ),
            axis=1,
            keepdims=True,
        )
        for k in range(2)
    ]
    expert_id = lax.broadcasted_iota(jnp.int32, (rows, experts), 1).astype(F32)
    chosen = [(route[k] == expert_id).astype(F32) for k in range(2)]
    hits = chosen[0] + chosen[1]
    row_id = lax.broadcasted_iota(jnp.int32, (rows, rows), 0)
    col_id = lax.broadcasted_iota(jnp.int32, (rows, rows), 1)
    earlier = (row_id > col_id).astype(BF16)
    prior = dot(earlier, hits.astype(BF16))
    slot_id = lax.broadcasted_iota(jnp.int32, (rows, experts * cap), 1).astype(F32)
    places = []
    for k in range(2):
        rank = jnp.sum(prior * chosen[k], axis=1, keepdims=True)
        target = route[k] * cap + rank
        places.append((target == slot_id).astype(F32))
    dispatch_map = (places[0] + places[1]).astype(BF16)

    diagonal = (
        lax.broadcasted_iota(jnp.int32, (rows, 128), 0)
        == lax.broadcasted_iota(jnp.int32, (rows, 128), 1)
    )

    def exchange(n, columns):
        for i, column in enumerate(columns):
            stat_send[n, i : i + 1, :] = jnp.sum(
                jnp.where(diagonal, column, 0.0), axis=0, keepdims=True
            )
        for r in (2, 1, 3):
            send(
                stat_send.at[n],
                stat_recv.at[n, r - 1],
                s_send.at[n, r - 1],
                s_recv.at[n, r - 1],
                {"tp": (tp + r) % n_tp},
            )

    def received(n, count):
        for r in range(1, n_tp):
            pltpu.make_async_copy(
                stat_recv.at[n, r - 1], stat_recv.at[n, r - 1], s_recv.at[n, r - 1]
            ).wait()
        parts = [stat_send[n]] + [stat_recv[n, r - 1] for r in range(1, n_tp)]
        return [
            [
                jnp.sum(jnp.where(diagonal, part[i : i + 1, :], 0.0), axis=1, keepdims=True)
                for i in range(count)
            ]
            for part in parts
        ]

    def norm_terms(n, values):
        mean_own = jnp.mean(values, axis=1, keepdims=True)
        spread_own = jnp.sum(jnp.square(values - mean_own), axis=1, keepdims=True)
        exchange(n, [mean_own, spread_own])
        stats = received(n, 2)
        mean = sum(s[0] for s in stats) / n_tp
        spread = sum(s[1] + share * jnp.square(s[0] - mean) for s in stats) / width
        return mean, lax.rsqrt(spread + norm_eps)

    for r in range(1, n_tp):
        waits[r].wait_recv()
    mixed = out_part[0].astype(F32)
    for r in range(1, n_tp):
        mixed = mixed + out_recv[r - 1].astype(F32)
    values = residual_scale * x_v[:, share_at].astype(F32) + mixed
    mean, scale = norm_terms(0, values)
    hidden = (values - mean) * scale * gmix_v[...]
    hid_v[...] = hidden
    hidden_bf = hidden.astype(BF16)

    z_buf[...] = (
        lax.dot_general(
            dispatch_map, hidden_bf, (((0,), (0,)), ((), ())), preferred_element_type=F32
        )
        .reshape(n_ep, slots, share)
        .astype(BF16)
    )
    z_recv_buf[0, core] = z_buf[ep]
    for k in range(CHUNKS):
        for i, offset in enumerate(offsets[k]):
            for c in (1, 0):
                if offset == 0 and c == 0:
                    continue
                target = ((chip + chips - offset) % chips) * CORES + (core + c) % CORES
                send(
                    z_buf.at[target],
                    z_recv_buf.at[k, i * CORES + core],
                    z_send.at[(k * len(offsets[k]) + i) * CORES + c],
                    z_recv.at[k],
                    {"ep": target},
                )

    group_logit = dot_t(hidden_bf, wgrp_v[...])
    expert_logit = dot_t(hidden_bf, wexp_v[...])
    columns = [jnp.sum(chosen[k] * expert_logit, axis=1, keepdims=True) for k in range(2)]
    columns += [group_logit[:, i : i + 1] for i in range(egroups)]
    exchange(1, columns)

    def wait_bytes(ref, sem):
        pltpu.make_async_copy(ref, ref, sem).wait()

    def gather(k):
        count = per_chunk - 1 if k == 0 else per_chunk
        wait_bytes(z_recv_buf.at[k, 0:count], z_recv.at[k])
        for r in (2, 1, 3):
            send(
                z_recv_buf.at[k],
                gather_buf.at[k, tp],
                x_send.at[k, r - 1],
                x_recv.at[k, r - 1],
                {"tp": (tp + r) % n_tp},
            )
        gather_buf[k, tp] = z_recv_buf[k]

    def experts_of(k):
        for r in range(1, n_tp):
            wait_bytes(gather_buf.at[k, 0], x_recv.at[k, r - 1])
        if k == 0:
            for name in ("wg", "wu", "wd"):
                loads[name].wait()
        lhs = [gather_buf[k, t].reshape(chunk_rows, share) for t in range(n_tp)]
        lhs = jnp.concatenate(lhs, axis=1)
        slot = lax.broadcasted_iota(jnp.int32, (chunk_rows, 1), 0) % slots
        acts = []
        for e in range(local_experts):
            gate = dot(lhs, wg_v[e])
            up = dot(lhs, wu_v[e])
            mine = slot // cap == e
            acts.append(jnp.where(mine, jax.nn.silu(gate) * up, 0.0).astype(BF16))
        act = jnp.concatenate(acts, axis=1)
        for r in (2, 1, 3, 0):
            q = (tp + r) % n_tp
            cols = pl.ds(pl.multiple_of(q * share, share), share)
            down_part[k, r] = dot(act, wd_v[:, cols]).astype(BF16)
            if r:
                send(
                    down_part.at[k, r],
                    down_recv.at[k, r - 1],
                    d_send.at[k, r - 1],
                    d_recv.at[k, r - 1],
                    {"tp": q},
                )

    def give_back(k):
        for r in range(1, n_tp):
            wait_bytes(down_recv.at[k, r - 1], d_recv.at[k, r - 1])
        total = down_part[k, 0].astype(F32)
        for r in range(1, n_tp):
            total = total + down_recv[k, r - 1].astype(F32)
        ret_send[k] = total.reshape(per_chunk, slots, share).astype(BF16)
        for i, offset in enumerate(offsets[k]):
            for c in (1, 0):
                to_core = (core + c) % CORES
                if offset == 0 and c == 0:
                    continue
                target = ((chip + offset) % chips) * CORES + to_core
                send(
                    ret_send.at[k, i * CORES + to_core],
                    ret_buf.at[ep],
                    r_send.at[(k * len(offsets[k]) + i) * CORES + c],
                    r_recv,
                    {"ep": target},
                )
        if k == 0:
            ret_buf[ep] = ret_send[0, core]

    gather(0)
    gather(1)
    experts_of(0)
    for k in range(2, CHUNKS):
        gather(k)
        experts_of(k - 1)
        give_back(k - 2)
    experts_of(CHUNKS - 1)
    give_back(CHUNKS - 2)

    parts = received(1, 2 + egroups)
    total = [sum(p[i] for p in parts) for i in range(2 + egroups)]
    pair = [jnp.exp(total[k]) for k in range(2)]
    group_exp = [jnp.exp(total[2 + i]) for i in range(egroups)]
    group_size = experts // egroups
    picked = sum(
        jnp.where(
            (route[0] >= i * group_size) & (route[0] < (i + 1) * group_size), group_exp[i], 0.0
        )
        for i in range(egroups)
    )
    group_prob = picked / sum(group_exp)
    pair_sum = pair[0] + pair[1]
    combine_map = sum(places[k] * (pair[k] / pair_sum * group_prob) for k in range(2))
    combine_map = combine_map.astype(BF16)
    loads["gmoe"].wait()

    give_back(CHUNKS - 1)

    wait_bytes(ret_buf.at[0 : n_ep - 1], r_recv)
    returned = ret_buf[...].reshape(n_ep * slots, share)
    values = residual_scale * hid_v[...] + dot(combine_map, returned)
    mean, scale = norm_terms(2, values)
    fin_v[...] = ((values - mean) * scale * gmoe_v[...]).astype(BF16)
    last = []
    for r in (2, 1, 3):
        last.append(
            send(
                fin_v,
                out_h.at[:, share_at],
                f_send.at[r - 1],
                f_recv.at[r - 1],
                {"tp": (tp + r) % n_tp},
            )
        )
    own_store = pltpu.make_async_copy(fin_v, out_h.at[:, share_at], f_send.at[n_tp - 1])
    own_store.start()
    for copy in last:
        copy.wait_recv()
    own_store.wait()
    store.wait()
    for copy in sends:
        copy.wait_send()


def per_device(
    n_ep,
    n_tp,
    x_in,
    state,
    routes,
    w_in,
    decay_rate,
    frequency,
    log_step,
    b_in,
    c_out,
    skip,
    w_out,
    gain_mix,
    w_group,
    w_expert,
    w_gate,
    w_up,
    w_down,
    gain_moe,
):
    rows, width = x_in.shape
    share = width // n_tp
    groups, entries = decay_rate.shape
    lanes = 2 * entries
    channels = skip.shape[0]
    experts = w_expert.shape[1]
    egroups = w_group.shape[1]
    local_experts, _, hidden_units = w_gate.shape
    cap = max(2, 4 * rows // experts)
    slots = local_experts * cap
    per_chunk = n_ep // CHUNKS
    args = (
        x_in,
        state.reshape(rows * groups, lanes),
        routes.T,
        w_in,
        decay_rate,
        frequency,
        log_step.reshape(1, groups),
        b_in.reshape(channels, lanes),
        c_out.reshape(channels, lanes),
        skip.reshape(channels // lanes, lanes),
        w_out,
        gain_mix.reshape(1, width),
        w_group.T,
        w_expert.T,
        w_gate,
        w_up,
        w_down.reshape(local_experts * hidden_units, width),
        gain_moe.reshape(1, width),
    )
    dma = pltpu.SemaphoreType.DMA
    peers = n_tp - 1
    scratch = [
        pltpu.VMEM((rows, width), BF16),
        pltpu.VMEM((rows * groups, lanes), F32),
        pltpu.VMEM(routes.shape[::-1], jnp.int32),
        pltpu.VMEM(w_in.shape, BF16),
        pltpu.VMEM(decay_rate.shape, F32),
        pltpu.VMEM(frequency.shape, F32),
        pltpu.VMEM((1, groups), F32),
        pltpu.VMEM((channels, lanes), F32),
        pltpu.VMEM((channels, lanes), F32),
        pltpu.VMEM((channels // lanes, lanes), F32),
        pltpu.VMEM(w_out.shape, BF16),
        pltpu.VMEM((1, share), F32),
        pltpu.VMEM((egroups, share), BF16),
        pltpu.VMEM((experts, share), BF16),
        pltpu.VMEM(w_gate.shape, BF16),
        pltpu.VMEM(w_up.shape, BF16),
        pltpu.VMEM((local_experts * hidden_units, width), BF16),
        pltpu.VMEM((1, share), F32),
        pltpu.VMEM((rows * groups, lanes), F32),
        pltpu.VMEM((n_tp, rows, share), BF16),
        pltpu.VMEM((peers, rows, share), BF16),
        pltpu.VMEM((rows, share), F32),
        pltpu.VMEM((3, 8, 128), F32),
        pltpu.VMEM((3, peers, 8, 128), F32),
        pltpu.VMEM((n_ep, slots, share), BF16),
        pltpu.VMEM((CHUNKS, per_chunk, slots, share), BF16),
        pltpu.VMEM((CHUNKS, n_tp, per_chunk, slots, share), BF16),
        pltpu.VMEM((CHUNKS, n_tp, per_chunk * slots, share), BF16),
        pltpu.VMEM((CHUNKS, peers, per_chunk * slots, share), BF16),
        pltpu.VMEM((CHUNKS, per_chunk, slots, share), BF16),
        pltpu.VMEM((n_ep, slots, share), BF16),
        pltpu.VMEM((rows, share), BF16),
        dma((len(args),)),
        dma,
        dma((peers,)),
        dma((peers,)),
        dma((3, peers)),
        dma((3, peers)),
        dma((n_ep,)),
        dma((CHUNKS,)),
        dma((CHUNKS, peers)),
        dma((CHUNKS, peers)),
        dma((CHUNKS, peers)),
        dma((CHUNKS, peers)),
        dma((n_ep,)),
        dma,
        dma((n_tp,)),
        dma((peers,)),
    ]
    any_space = pl.BlockSpec(memory_space=pl.ANY)
    out, new_state = pl.pallas_call(
        functools.partial(layer_kernel, n_ep, n_tp),
        out_shape=(
            jax.ShapeDtypeStruct((rows, width), BF16),
            jax.ShapeDtypeStruct((rows * groups, lanes), F32),
        ),
        in_specs=[any_space] * len(args),
        out_specs=(any_space, any_space),
        scratch_shapes=scratch,
        compiler_params=pltpu.CompilerParams(
            collective_id=0, has_side_effects=True, vmem_limit_bytes=60 * 1024 * 1024
        ),
        name="layer",
    )(*args)
    return out, new_state.reshape(state.shape)


def solution(mesh):
    in_specs = (
        P(("grp", "ep"), None),
        P(("grp", "ep"), "tp", None),
        P(("grp", "ep"), None),
        P(None, "tp"),
        P("tp", None),
        P("tp", None),
        P("tp"),
        P("tp", None, None),
        P("tp", None, None),
        P("tp"),
        P("tp", None),
        P(),
        P(),
        P(),
        P("ep", None, "tp"),
        P("ep", None, "tp"),
        P("ep", "tp", None),
        P(),
    )
    out_specs = (P(("grp", "ep"), None), P(("grp", "ep"), "tp", None))
    return jax.shard_map(
        functools.partial(per_device, mesh.shape["ep"], mesh.shape["tp"]),
        mesh=mesh,
        in_specs=in_specs,
        out_specs=out_specs,
        check_vma=False,
    )
```

```python
import functools

import jax
import jax.numpy as jnp
from jax import lax
from jax.experimental import pallas as pl
from jax.experimental.pallas import tpu as pltpu
from jax.sharding import PartitionSpec as P

residual_scale = 8.0**0.25
norm_eps = 1e-05
CORES = 2
CHUNKS = 4
F32 = jnp.float32
BF16 = jnp.bfloat16
MESH = pl.DeviceIdType.MESH


def dot(a, b):
    return jnp.dot(a, b, preferred_element_type=F32)


def dot_t(a, b):
    return lax.dot_general(a, b, (((1,), (1,)), ((), ())), preferred_element_type=F32)


def chip_offsets(chips):
    far_first = [chips // 2]
    for step in range(chips // 2 - 1, 0, -1):
        far_first += [step, chips - step]
    far_first.append(0)
    size = chips // CHUNKS
    first = far_first[-1 - size : -1]
    rest = far_first[: -1 - size] + [0]
    return [first] + [rest[k * size : (k + 1) * size] for k in range(CHUNKS - 1)]


def layer_kernel(
    n_ep,
    n_tp,
    x_h,
    state_h,
    routes_h,
    win_h,
    decay_h,
    freq_h,
    lstep_h,
    b_h,
    c_h,
    skip_h,
    wout_h,
    gmix_h,
    wgrp_h,
    wexp_h,
    wg_h,
    wu_h,
    wd_h,
    out_h,
    ns_h,
    x_v,
    state_v,
    routes_v,
    win_v,
    decay_v,
    freq_v,
    lstep_v,
    b_v,
    c_v,
    skip_v,
    wout_v,
    gmix_v,
    wgrp_v,
    wexp_v,
    wg_v,
    wu_v,
    wd_v,
    ns_v,
    out_part,
    out_recv,
    hid_v,
    stat_send,
    stat_recv,
    z_buf,
    z_recv_buf,
    gather_buf,
    down_part,
    down_recv,
    ret_send,
    ret_buf,
    fin_v,
    load_sem,
    store_sem,
    a_send,
    a_recv,
    s_send,
    s_recv,
    z_send,
    z_recv,
    x_send,
    x_recv,
    d_send,
    d_recv,
    r_send,
    r_recv,
    f_send,
    f_recv,
):
    ep = lax.axis_index("ep")
    tp = lax.axis_index("tp")
    chips = n_ep // CORES
    chip = ep // CORES
    core = ep % CORES
    rows, width = x_v.shape
    share = width // n_tp
    entries = decay_v.shape[1]
    lanes = 2 * entries
    groups = decay_v.shape[0]
    group_width = b_v.shape[0] // groups
    experts = wexp_v.shape[0]
    egroups = wgrp_v.shape[0]
    local_experts = wg_v.shape[0]
    cap = z_buf.shape[1] // local_experts
    slots = z_buf.shape[1]
    offsets = chip_offsets(chips)
    per_chunk = n_ep // CHUNKS
    chunk_rows = per_chunk * slots
    share_at = pl.ds(pl.multiple_of(tp * share, share), share)

    loads = {}
    pairs = (
        ("x", x_h, x_v),
        ("win", win_h, win_v),
        ("decay", decay_h, decay_v),
        ("freq", freq_h, freq_v),
        ("lstep", lstep_h, lstep_v),
        ("b", b_h, b_v),
        ("c", c_h, c_v),
        ("state", state_h, state_v),
        ("skip", skip_h, skip_v),
        ("wout", wout_h, wout_v),
        ("gmix", gmix_h, gmix_v),
        ("routes", routes_h, routes_v),
        ("wgrp", wgrp_h.at[:, share_at], wgrp_v),
        ("wexp", wexp_h.at[:, share_at], wexp_v),
        ("wg", wg_h, wg_v),
        ("wu", wu_h, wu_v),
        ("wd", wd_h, wd_v),
    )
    for i, (name, src, dst) in enumerate(pairs):
        loads[name] = pltpu.make_async_copy(src, dst, load_sem.at[i])
        loads[name].start()

    barrier = pltpu.get_barrier_semaphore()

    def greet_ep(i, _):
        step = n_ep // 2 + jnp.where(i % 2 == 0, i // 2, -(i // 2) - 1)
        peer = (ep + step) % n_ep
        pl.semaphore_signal(barrier, inc=1, device_id={"ep": peer}, device_id_type=MESH)
        return 0

    for r in range(1, n_tp):
        pl.semaphore_signal(
            barrier, inc=1, device_id={"tp": (tp + r) % n_tp}, device_id_type=MESH
        )
    lax.fori_loop(0, n_ep - 1, greet_ep, 0)

    sends = []

    def send(src, dst, send_sem, recv_sem, target):
        copy = pltpu.make_async_remote_copy(
            src_ref=src,
            dst_ref=dst,
            send_sem=send_sem,
            recv_sem=recv_sem,
            device_id=target,
            device_id_type=MESH,
        )
        copy.start()
        sends.append(copy)
        return copy

    for name in ("decay", "freq", "lstep", "b", "c"):
        loads[name].wait()
    eye = (
        lax.broadcasted_iota(jnp.int32, (groups, groups), 0)
        == lax.broadcasted_iota(jnp.int32, (groups, groups), 1)
    )
    log_step = jnp.sum(jnp.where(eye, lstep_v[...], 0.0), axis=1, keepdims=True)
    step_size = jnp.exp(log_step)
    decay = decay_v[...]
    freq = freq_v[...]
    lam_real = -decay
    magnitude = jnp.exp(lam_real * step_size)
    angle = freq * step_size
    bar_real = magnitude * jnp.cos(angle)
    bar_imag = magnitude * jnp.sin(angle)
    minus_real = bar_real - 1.0
    modulus = lam_real * lam_real + freq * freq
    ratio_real = (minus_real * lam_real + bar_imag * freq) / modulus
    ratio_imag = (bar_imag * lam_real - minus_real * freq) / modulus
    bar_same = jnp.concatenate([bar_real, bar_real], axis=1)
    bar_cross = jnp.concatenate([-bar_imag, bar_imag], axis=1)
    ratio_same = jnp.concatenate([ratio_real, ratio_real], axis=1)
    ratio_cross = jnp.concatenate([-ratio_imag, ratio_imag], axis=1)

    loads["x"].wait()
    loads["win"].wait()
    mix_input = dot(x_v[...], win_v[...]).astype(BF16)
    loads["skip"].wait()
    loads["state"].wait()

    per_block = lanes // group_width
    block_lanes = per_block * lanes
    own_group = (
        lax.broadcasted_iota(jnp.int32, (lanes, block_lanes), 0) // group_width
        == lax.broadcasted_iota(jnp.int32, (lanes, block_lanes), 1) // lanes
    )
    sign = jnp.where(lax.broadcasted_iota(jnp.int32, (1, lanes), 1) < entries, 1.0, -1.0)
    acts = []
    for j in range(groups // per_block):
        channels = slice(j * lanes, (j + 1) * lanes)
        bars = []
        for g in range(j * per_block, (j + 1) * per_block):
            b_g = b_v[g * group_width : (g + 1) * group_width, :]
            bars.append(
                b_g * ratio_same[g : g + 1, :]
                + pltpu.roll(b_g, entries, 1) * ratio_cross[g : g + 1, :]
            )
        b_bar = jnp.concatenate(bars, axis=0)
        b_wide = jnp.where(own_group, jnp.concatenate([b_bar] * per_block, axis=1), 0.0)
        u_j = mix_input[:, channels]
        forcing = dot(u_j, b_wide.astype(BF16))
        news = []
        for i in range(per_block):
            g = j * per_block + i
            old = state_v[pl.ds(g, rows, stride=groups), :]
            new = (
                old * bar_same[g : g + 1, :]
                + pltpu.roll(old, entries, 1) * bar_cross[g : g + 1, :]
                + forcing[:, i * lanes : (i + 1) * lanes]
            )
            ns_v[pl.ds(g, rows, stride=groups), :] = new
            news.append(new.astype(BF16))
        c_j = c_v[channels, :] * sign
        c_wide = jnp.where(own_group, jnp.concatenate([c_j] * per_block, axis=1), 0.0)
        y = dot_t(jnp.concatenate(news, axis=1), c_wide.astype(BF16))
        y = y + skip_v[j : j + 1, :] * u_j.astype(F32)
        acts.append(jax.nn.gelu(y).astype(BF16))
    store = pltpu.make_async_copy(ns_v, ns_h, store_sem)
    store.start()
    act_mix = jnp.concatenate(acts, axis=1)

    loads["wout"].wait()
    for r in (2, 1, 3, 0):
        q = (tp + r) % n_tp
        cols = pl.ds(pl.multiple_of(q * share, share), share)
        out_part[r] = dot(act_mix, wout_v[:, cols]).astype(BF16)
    pl.semaphore_wait(barrier, n_ep - 1 + n_tp - 1)
    waits = {}
    for r in (2, 1, 3):
        waits[r] = send(
            out_part.at[r],
            out_recv.at[r - 1],
            a_send.at[r - 1],
            a_recv.at[r - 1],
            {"tp": (tp + r) % n_tp},
        )

    for name in ("routes", "gmix", "wgrp", "wexp"):
        loads[name].wait()
    route = [
        jnp.sum(
            jnp.where(
                lax.broadcasted_iota(jnp.int32, (rows, rows), 0)
                == lax.broadcasted_iota(jnp.int32, (rows, rows), 1),
                routes_v[k : k + 1, :].astype(F32),
                0.0,
            ),
            axis=1,
            keepdims=True,
        )
        for k in range(2)
    ]
    expert_id = lax.broadcasted_iota(jnp.int32, (rows, experts), 1).astype(F32)
    chosen = [(route[k] == expert_id).astype(F32) for k in range(2)]
    hits = chosen[0] + chosen[1]
    row_id = lax.broadcasted_iota(jnp.int32, (rows, rows), 0)
    col_id = lax.broadcasted_iota(jnp.int32, (rows, rows), 1)
    earlier = (row_id > col_id).astype(BF16)
    prior = dot(earlier, hits.astype(BF16))
    slot_id = lax.broadcasted_iota(jnp.int32, (rows, experts * cap), 1).astype(F32)
    places = []
    for k in range(2):
        rank = jnp.sum(prior * chosen[k], axis=1, keepdims=True)
        target = route[k] * cap + rank
        places.append((target == slot_id).astype(F32))
    dispatch_map = (places[0] + places[1]).astype(BF16)

    diagonal = (
        lax.broadcasted_iota(jnp.int32, (rows, 128), 0)
        == lax.broadcasted_iota(jnp.int32, (rows, 128), 1)
    )

    def exchange(n, columns):
        for i, column in enumerate(columns):
            stat_send[n, i : i + 1, :] = jnp.sum(
                jnp.where(diagonal, column, 0.0), axis=0, keepdims=True
            )
        for r in (2, 1, 3):
            send(
                stat_send.at[n],
                stat_recv.at[n, r - 1],
                s_send.at[n, r - 1],
                s_recv.at[n, r - 1],
                {"tp": (tp + r) % n_tp},
            )

    def received(n, count):
        for r in range(1, n_tp):
            pltpu.make_async_copy(
                stat_recv.at[n, r - 1], stat_recv.at[n, r - 1], s_recv.at[n, r - 1]
            ).wait()
        parts = [stat_send[n]] + [stat_recv[n, r - 1] for r in range(1, n_tp)]
        return [
            [
                jnp.sum(jnp.where(diagonal, part[i : i + 1, :], 0.0), axis=1, keepdims=True)
                for i in range(count)
            ]
            for part in parts
        ]

    shift = residual_scale * jnp.mean(x_v[...].astype(F32), axis=1, keepdims=True)
    base = residual_scale * x_v[:, share_at].astype(F32) - shift

    for r in range(1, n_tp):
        waits[r].wait_recv()
    mixed = out_part[0].astype(F32)
    for r in range(1, n_tp):
        mixed = mixed + out_recv[r - 1].astype(F32)
    values = base + mixed

    z_buf[...] = (
        lax.dot_general(
            dispatch_map, values.astype(BF16), (((0,), (0,)), ((), ())), preferred_element_type=F32
        )
        .reshape(n_ep, slots, share)
        .astype(BF16)
    )
    z_recv_buf[CHUNKS - 1, per_chunk - CORES + core] = z_buf[ep]
    for k in range(CHUNKS):
        for i, offset in enumerate(offsets[k]):
            for c in (1, 0):
                if offset == 0 and c == 0:
                    continue
                target = ((chip + chips - offset) % chips) * CORES + (core + c) % CORES
                send(
                    z_buf.at[target],
                    z_recv_buf.at[k, i * CORES + core],
                    z_send.at[(k * len(offsets[k]) + i) * CORES + c],
                    z_recv.at[k],
                    {"ep": target},
                )

    mean_own = jnp.mean(values, axis=1, keepdims=True)
    spread_own = jnp.sum(jnp.square(values - mean_own), axis=1, keepdims=True)
    exchange(0, [mean_own, spread_own])
    hid_v[...] = values

    def wait_bytes(ref, sem):
        pltpu.make_async_copy(ref, ref, sem).wait()

    def gather(k):
        count = per_chunk - 1 if k == CHUNKS - 1 else per_chunk
        wait_bytes(z_recv_buf.at[k, 0:count], z_recv.at[k])
        for r in (2, 1, 3):
            send(
                z_recv_buf.at[k],
                gather_buf.at[k, tp],
                x_send.at[k, r - 1],
                x_recv.at[k, r - 1],
                {"tp": (tp + r) % n_tp},
            )
        gather_buf[k, tp] = z_recv_buf[k]

    def experts_of(k):
        for r in range(1, n_tp):
            wait_bytes(gather_buf.at[k, 0], x_recv.at[k, r - 1])
        if k == 0:
            for name in ("wg", "wu", "wd"):
                loads[name].wait()
        parts = [gather_buf[k, t].astype(F32).reshape(chunk_rows, share) for t in range(n_tp)]
        mean = sum(jnp.sum(p, axis=1, keepdims=True) for p in parts) / width
        parts = [p - mean for p in parts]
        spread = sum(jnp.sum(jnp.square(p), axis=1, keepdims=True) for p in parts) / width
        scale = lax.rsqrt(spread + norm_eps)
        lhs = jnp.concatenate(
            [
                (p * scale * gmix_v[:, t * share : (t + 1) * share]).astype(BF16)
                for t, p in enumerate(parts)
            ],
            axis=1,
        )
        slot = lax.broadcasted_iota(jnp.int32, (chunk_rows, 1), 0) % slots
        acts = []
        for e in range(local_experts):
            gate = dot(lhs, wg_v[e])
            up = dot(lhs, wu_v[e])
            mine = slot // cap == e
            acts.append(jnp.where(mine, jax.nn.silu(gate) * up, 0.0).astype(BF16))
        act = jnp.concatenate(acts, axis=1)
        for r in (2, 1, 3, 0):
            q = (tp + r) % n_tp
            cols = pl.ds(pl.multiple_of(q * share, share), share)
            down_part[k, r] = dot(act, wd_v[:, cols]).astype(BF16)
            if r:
                send(
                    down_part.at[k, r],
                    down_recv.at[k, r - 1],
                    d_send.at[k, r - 1],
                    d_recv.at[k, r - 1],
                    {"tp": q},
                )

    def give_back(k):
        for r in range(1, n_tp):
            wait_bytes(down_recv.at[k, r - 1], d_recv.at[k, r - 1])
        total = down_part[k, 0].astype(F32)
        for r in range(1, n_tp):
            total = total + down_recv[k, r - 1].astype(F32)
        ret_send[k] = total.reshape(per_chunk, slots, share).astype(BF16)
        for i, offset in enumerate(offsets[k]):
            for c in (1, 0):
                to_core = (core + c) % CORES
                if offset == 0 and c == 0:
                    continue
                target = ((chip + offset) % chips) * CORES + to_core
                send(
                    ret_send.at[k, i * CORES + to_core],
                    ret_buf.at[ep],
                    r_send.at[(k * len(offsets[k]) + i) * CORES + c],
                    r_recv,
                    {"ep": target},
                )
        if k == CHUNKS - 1:
            ret_buf[ep] = ret_send[k, per_chunk - CORES + core]

    gather(0)

    stats = received(0, 2)
    mean = sum(s[0] for s in stats) / n_tp
    spread = sum(s[1] + share * jnp.square(s[0] - mean) for s in stats) / width
    hidden = (hid_v[...] - mean) * lax.rsqrt(spread + norm_eps) * gmix_v[:, share_at]
    hid_v[...] = hidden
    hidden_bf = hidden.astype(BF16)

    group_logit = dot_t(hidden_bf, wgrp_v[...])
    expert_logit = dot_t(hidden_bf, wexp_v[...])
    columns = [jnp.sum(chosen[k] * expert_logit, axis=1, keepdims=True) for k in range(2)]
    columns += [group_logit[:, i : i + 1] for i in range(egroups)]
    exchange(1, columns)

    experts_of(0)
    gather(1)
    give_back(0)
    gather(2)
    gather(3)
    experts_of(1)
    experts_of(2)
    give_back(1)
    experts_of(3)
    give_back(2)

    parts = received(1, 2 + egroups)
    total = [sum(p[i] for p in parts) for i in range(2 + egroups)]
    pair = [jnp.exp(total[k]) for k in range(2)]
    group_exp = [jnp.exp(total[2 + i]) for i in range(egroups)]
    group_size = experts // egroups
    picked = sum(
        jnp.where(
            (route[0] >= i * group_size) & (route[0] < (i + 1) * group_size), group_exp[i], 0.0
        )
        for i in range(egroups)
    )
    group_prob = picked / sum(group_exp)
    pair_sum = pair[0] + pair[1]
    combine_map = sum(places[k] * (pair[k] / pair_sum * group_prob) for k in range(2))
    combine_map = combine_map.astype(BF16)

    give_back(CHUNKS - 1)

    wait_bytes(ret_buf.at[0 : n_ep - 1], r_recv)
    returned = ret_buf[...].reshape(n_ep * slots, share)
    values = residual_scale * hid_v[...] + dot(combine_map, returned)
    fin_v[...] = values.astype(BF16)
    last = []
    for r in (2, 1, 3):
        last.append(
            send(
                fin_v,
                out_h.at[:, share_at],
                f_send.at[r - 1],
                f_recv.at[r - 1],
                {"tp": (tp + r) % n_tp},
            )
        )
    own_store = pltpu.make_async_copy(fin_v, out_h.at[:, share_at], f_send.at[n_tp - 1])
    own_store.start()
    for copy in last:
        copy.wait_recv()
    own_store.wait()
    store.wait()
    for copy in sends:
        copy.wait_send()


def finish_kernel(
    pieces,
    raw_h,
    ns_h,
    gain_h,
    out_h,
    new_h,
    raw_v,
    ns_v,
    gain_v,
    out_v,
    load_sem,
    store_sem,
    in_sem,
    out_sem,
):
    size = ns_v.shape[0] // pieces
    raw = pltpu.make_async_copy(raw_h, raw_v, load_sem.at[0])
    gain = pltpu.make_async_copy(gain_h, gain_v, load_sem.at[1])
    raw.start()
    gain.start()
    ins, outs = [], []
    for i in range(pieces):
        part = pl.ds(i * size, size)
        ins.append(pltpu.make_async_copy(ns_h.at[part], ns_v.at[part], in_sem.at[i]))
        outs.append(pltpu.make_async_copy(ns_v.at[part], new_h.at[part], out_sem.at[i]))
        ins[i].start()
    raw.wait()
    gain.wait()
    values = raw_v[...].astype(F32)
    centred = values - jnp.mean(values, axis=1, keepdims=True)
    spread = jnp.mean(jnp.square(centred), axis=1, keepdims=True)
    out_v[...] = (centred * lax.rsqrt(spread + norm_eps) * gain_v[...]).astype(BF16)
    store = pltpu.make_async_copy(out_v, out_h, store_sem)
    store.start()
    for i in range(pieces):
        ins[i].wait()
        outs[i].start()
    for copy in outs:
        copy.wait()
    store.wait()


def per_device(
    n_ep,
    n_tp,
    x_in,
    state,
    routes,
    w_in,
    decay_rate,
    frequency,
    log_step,
    b_in,
    c_out,
    skip,
    w_out,
    gain_mix,
    w_group,
    w_expert,
    w_gate,
    w_up,
    w_down,
    gain_moe,
):
    rows, width = x_in.shape
    share = width // n_tp
    groups, entries = decay_rate.shape
    lanes = 2 * entries
    channels = skip.shape[0]
    experts = w_expert.shape[1]
    egroups = w_group.shape[1]
    local_experts, _, hidden_units = w_gate.shape
    cap = max(2, 4 * rows // experts)
    slots = local_experts * cap
    per_chunk = n_ep // CHUNKS
    args = (
        x_in,
        state.reshape(rows * groups, lanes),
        routes.T,
        w_in,
        decay_rate,
        frequency,
        log_step.reshape(1, groups),
        b_in.reshape(channels, lanes),
        c_out.reshape(channels, lanes),
        skip.reshape(channels // lanes, lanes),
        w_out,
        gain_mix.reshape(1, width),
        w_group.T,
        w_expert.T,
        w_gate,
        w_up,
        w_down.reshape(local_experts * hidden_units, width),
    )
    dma = pltpu.SemaphoreType.DMA
    peers = n_tp - 1
    scratch = [
        pltpu.VMEM((rows, width), BF16),
        pltpu.VMEM((rows * groups, lanes), F32),
        pltpu.VMEM(routes.shape[::-1], jnp.int32),
        pltpu.VMEM(w_in.shape, BF16),
        pltpu.VMEM(decay_rate.shape, F32),
        pltpu.VMEM(frequency.shape, F32),
        pltpu.VMEM((1, groups), F32),
        pltpu.VMEM((channels, lanes), F32),
        pltpu.VMEM((channels, lanes), F32),
        pltpu.VMEM((channels // lanes, lanes), F32),
        pltpu.VMEM(w_out.shape, BF16),
        pltpu.VMEM((1, width), F32),
        pltpu.VMEM((egroups, share), BF16),
        pltpu.VMEM((experts, share), BF16),
        pltpu.VMEM(w_gate.shape, BF16),
        pltpu.VMEM(w_up.shape, BF16),
        pltpu.VMEM((local_experts * hidden_units, width), BF16),
        pltpu.VMEM((rows * groups, lanes), F32),
        pltpu.VMEM((n_tp, rows, share), BF16),
        pltpu.VMEM((peers, rows, share), BF16),
        pltpu.VMEM((rows, share), F32),
        pltpu.VMEM((2, 8, 128), F32),
        pltpu.VMEM((2, peers, 8, 128), F32),
        pltpu.VMEM((n_ep, slots, share), BF16),
        pltpu.VMEM((CHUNKS, per_chunk, slots, share), BF16),
        pltpu.VMEM((CHUNKS, n_tp, per_chunk, slots, share), BF16),
        pltpu.VMEM((CHUNKS, n_tp, per_chunk * slots, share), BF16),
        pltpu.VMEM((CHUNKS, peers, per_chunk * slots, share), BF16),
        pltpu.VMEM((CHUNKS, per_chunk, slots, share), BF16),
        pltpu.VMEM((n_ep, slots, share), BF16),
        pltpu.VMEM((rows, share), BF16),
        dma((len(args),)),
        dma,
        dma((peers,)),
        dma((peers,)),
        dma((2, peers)),
        dma((2, peers)),
        dma((n_ep,)),
        dma((CHUNKS,)),
        dma((CHUNKS, peers)),
        dma((CHUNKS, peers)),
        dma((CHUNKS, peers)),
        dma((CHUNKS, peers)),
        dma((n_ep,)),
        dma,
        dma((n_tp,)),
        dma((peers,)),
    ]
    any_space = pl.BlockSpec(memory_space=pl.ANY)
    raw, new_state = pl.pallas_call(
        functools.partial(layer_kernel, n_ep, n_tp),
        out_shape=(
            jax.ShapeDtypeStruct((rows, width), BF16),
            jax.ShapeDtypeStruct((rows * groups, lanes), F32),
        ),
        in_specs=[any_space] * len(args),
        out_specs=(any_space, any_space),
        scratch_shapes=scratch,
        compiler_params=pltpu.CompilerParams(
            collective_id=0, has_side_effects=True, vmem_limit_bytes=60 * 1024 * 1024
        ),
        name="layer",
    )(*args)
    pieces = 4
    out, new_state = pl.pallas_call(
        functools.partial(finish_kernel, pieces),
        out_shape=(
            jax.ShapeDtypeStruct((rows, width), BF16),
            jax.ShapeDtypeStruct((rows * groups, lanes), F32),
        ),
        in_specs=[any_space] * 3,
        out_specs=(any_space, any_space),
        scratch_shapes=[
            pltpu.VMEM((rows, width), BF16),
            pltpu.VMEM((rows * groups, lanes), F32),
            pltpu.VMEM((1, width), F32),
            pltpu.VMEM((rows, width), BF16),
            dma((2,)),
            dma,
            dma((pieces,)),
            dma((pieces,)),
        ],
        name="finish",
    )(raw, new_state, gain_moe.reshape(1, width))
    return out, new_state.reshape(state.shape)


def solution(mesh):
    in_specs = (
        P(("grp", "ep"), None),
        P(("grp", "ep"), "tp", None),
        P(("grp", "ep"), None),
        P(None, "tp"),
        P("tp", None),
        P("tp", None),
        P("tp"),
        P("tp", None, None),
        P("tp", None, None),
        P("tp"),
        P("tp", None),
        P(),
        P(),
        P(),
        P("ep", None, "tp"),
        P("ep", None, "tp"),
        P("ep", "tp", None),
        P(),
    )
    out_specs = (P(("grp", "ep"), None), P(("grp", "ep"), "tp", None))
    return jax.shard_map(
        functools.partial(per_device, mesh.shape["ep"], mesh.shape["tp"]),
        mesh=mesh,
        in_specs=in_specs,
        out_specs=out_specs,
        check_vma=False,
    )
```

```python
import functools

import jax
import jax.numpy as jnp
from jax import lax
from jax.experimental import pallas as pl
from jax.experimental.pallas import tpu as pltpu
from jax.sharding import PartitionSpec as P

residual_scale = 8.0**0.25
norm_eps = 1e-05
CORES = 2
NEAR = 1
ARC = 5
SCHEDULE = ("D0", "D1", "G0", "H0", "E0", "G1", "G2", "B0", "E1", "G3", "E2", "B1", "E3", "B2", "W0", "B3")
F32 = jnp.float32
BF16 = jnp.bfloat16
MESH = pl.DeviceIdType.MESH


def dot(a, b):
    return jnp.dot(a, b, preferred_element_type=F32)


def dot_t(a, b):
    return lax.dot_general(a, b, (((1,), (1,)), ((), ())), preferred_element_type=F32)


def layer_kernel(
    n_ep,
    n_tp,
    x_h,
    state_h,
    routes_h,
    win_h,
    decay_h,
    freq_h,
    lstep_h,
    b_h,
    c_h,
    skip_h,
    wout_h,
    gmix_h,
    wgrp_h,
    wexp_h,
    wg_h,
    wu_h,
    wd_h,
    out_h,
    ns_h,
    x_v,
    state_v,
    routes_v,
    win_v,
    decay_v,
    freq_v,
    lstep_v,
    b_v,
    c_v,
    skip_v,
    wout_v,
    gmix_v,
    wgrp_v,
    wexp_v,
    wg_v,
    wu_v,
    wd_v,
    ns_v,
    out_part,
    out_recv,
    hid_v,
    stat_send,
    stat_recv,
    z_buf,
    z_recv_buf,
    gather_buf,
    down_part,
    down_recv,
    ret_send,
    ret_buf,
    fin_v,
    load_sem,
    store_sem,
    a_send,
    a_recv,
    s_send,
    s_recv,
    z_send,
    z_recv,
    x_send,
    x_recv,
    d_send,
    d_recv,
    r_send,
    r_recv,
    l_send,
    l_recv,
    o_send,
):
    ep = lax.axis_index("ep")
    tp = lax.axis_index("tp")
    chips = n_ep // CORES
    chip = ep // CORES
    core = ep % CORES
    rows, width = x_v.shape
    share = width // n_tp
    entries = decay_v.shape[1]
    lanes = 2 * entries
    groups = decay_v.shape[0]
    group_width = b_v.shape[0] // groups
    experts = wexp_v.shape[0]
    egroups = wgrp_v.shape[0]
    local_experts = wg_v.shape[0]
    cap = z_buf.shape[1] // local_experts
    slots = z_buf.shape[1]
    arc = chips - 2 * NEAR - 1
    near = [offset for step in range(1, NEAR + 1) for offset in (step, -step)] + [0]
    far = sorted(range(NEAR + 1, chips - NEAR), key=lambda offset: abs(offset - chips // 2))
    counts = [len(near) * CORES]
    counts += [min(ARC, arc - i) * CORES for i in range(0, arc, ARC)]
    chunks = len(counts)
    starts = [sum(counts[:k]) for k in range(chunks)]
    blocks = [pl.ds(starts[k], counts[k]) for k in range(chunks)]
    sums = [pl.ds(starts[k] * slots, counts[k] * slots) for k in range(chunks)]
    remote = [counts[0] - 1] + counts[1:]
    home = len(near) * CORES - CORES + core

    def wrapped(host):
        after = (host + chips - NEAR - 1) % chips
        return (chips - NEAR - 1 - host) * (1 - after // (arc - 1))

    right, left, opposite = (tp + 1) % n_tp, (tp + n_tp - 1) % n_tp, (tp + 2) % n_tp
    share_at = pl.ds(pl.multiple_of(tp * share, share), share)

    loads = {}
    pairs = (
        ("x", x_h, x_v),
        ("win", win_h, win_v),
        ("decay", decay_h, decay_v),
        ("freq", freq_h, freq_v),
        ("lstep", lstep_h, lstep_v),
        ("b", b_h, b_v),
        ("c", c_h, c_v),
        ("state", state_h, state_v),
        ("skip", skip_h, skip_v),
        ("wout", wout_h, wout_v),
        ("gmix", gmix_h, gmix_v),
        ("routes", routes_h, routes_v),
        ("wgrp", wgrp_h.at[:, share_at], wgrp_v),
        ("wexp", wexp_h.at[:, share_at], wexp_v),
        ("wg", wg_h, wg_v),
        ("wu", wu_h, wu_v),
        ("wd", wd_h, wd_v),
    )
    for i, (name, src, dst) in enumerate(pairs):
        loads[name] = pltpu.make_async_copy(src, dst, load_sem.at[i])
        loads[name].start()

    barrier = pltpu.get_barrier_semaphore()

    def greet_ep(i, _):
        step = n_ep // 2 + jnp.where(i % 2 == 0, i // 2, -(i // 2) - 1)
        peer = (ep + step) % n_ep
        pl.semaphore_signal(barrier, inc=1, device_id={"ep": peer}, device_id_type=MESH)
        return 0

    for r in range(1, n_tp):
        pl.semaphore_signal(
            barrier, inc=1, device_id={"tp": (tp + r) % n_tp}, device_id_type=MESH
        )
    lax.fori_loop(0, n_ep - 1, greet_ep, 0)

    def send(src, dst, send_sem, recv_sem, target):
        copy = pltpu.make_async_remote_copy(
            src_ref=src,
            dst_ref=dst,
            send_sem=send_sem,
            recv_sem=recv_sem,
            device_id=target,
            device_id_type=MESH,
        )
        copy.start()
        return copy

    def wait_bytes(ref, sem):
        pltpu.make_async_copy(ref, ref, sem).wait()

    for name in ("decay", "freq", "lstep", "b", "c"):
        loads[name].wait()
    eye = (
        lax.broadcasted_iota(jnp.int32, (groups, groups), 0)
        == lax.broadcasted_iota(jnp.int32, (groups, groups), 1)
    )
    log_step = jnp.sum(jnp.where(eye, lstep_v[...], 0.0), axis=1, keepdims=True)
    step_size = jnp.exp(log_step)
    decay = decay_v[...]
    freq = freq_v[...]
    lam_real = -decay
    magnitude = jnp.exp(lam_real * step_size)
    angle = freq * step_size
    bar_real = magnitude * jnp.cos(angle)
    bar_imag = magnitude * jnp.sin(angle)
    minus_real = bar_real - 1.0
    modulus = lam_real * lam_real + freq * freq
    ratio_real = (minus_real * lam_real + bar_imag * freq) / modulus
    ratio_imag = (bar_imag * lam_real - minus_real * freq) / modulus
    bar_same = jnp.concatenate([bar_real, bar_real], axis=1)
    bar_cross = jnp.concatenate([-bar_imag, bar_imag], axis=1)
    ratio_same = jnp.concatenate([ratio_real, ratio_real], axis=1)
    ratio_cross = jnp.concatenate([-ratio_imag, ratio_imag], axis=1)

    loads["x"].wait()
    loads["win"].wait()
    mix_input = dot(x_v[...], win_v[...]).astype(BF16)
    loads["skip"].wait()
    loads["state"].wait()

    per_block = lanes // group_width
    block_lanes = per_block * lanes
    own_group = (
        lax.broadcasted_iota(jnp.int32, (lanes, block_lanes), 0) // group_width
        == lax.broadcasted_iota(jnp.int32, (lanes, block_lanes), 1) // lanes
    )
    sign = jnp.where(lax.broadcasted_iota(jnp.int32, (1, lanes), 1) < entries, 1.0, -1.0)
    acts = []
    for j in range(groups // per_block):
        channels = slice(j * lanes, (j + 1) * lanes)
        bars = []
        for g in range(j * per_block, (j + 1) * per_block):
            b_g = b_v[g * group_width : (g + 1) * group_width, :]
            bars.append(
                b_g * ratio_same[g : g + 1, :]
                + pltpu.roll(b_g, entries, 1) * ratio_cross[g : g + 1, :]
            )
        b_bar = jnp.concatenate(bars, axis=0)
        b_wide = jnp.where(own_group, jnp.concatenate([b_bar] * per_block, axis=1), 0.0)
        u_j = mix_input[:, channels]
        forcing = dot(u_j, b_wide.astype(BF16))
        news = []
        for i in range(per_block):
            g = j * per_block + i
            old = state_v[pl.ds(g, rows, stride=groups), :]
            new = (
                old * bar_same[g : g + 1, :]
                + pltpu.roll(old, entries, 1) * bar_cross[g : g + 1, :]
                + forcing[:, i * lanes : (i + 1) * lanes]
            )
            ns_v[pl.ds(g, rows, stride=groups), :] = new
            news.append(new.astype(BF16))
        c_j = c_v[channels, :] * sign
        c_wide = jnp.where(own_group, jnp.concatenate([c_j] * per_block, axis=1), 0.0)
        y = dot_t(jnp.concatenate(news, axis=1), c_wide.astype(BF16))
        y = y + skip_v[j : j + 1, :] * u_j.astype(F32)
        acts.append(jax.nn.gelu(y).astype(BF16))
    store = pltpu.make_async_copy(ns_v, ns_h, store_sem)
    store.start()
    act_mix = jnp.concatenate(acts, axis=1)

    loads["wout"].wait()
    for r in (2, 1, 3, 0):
        q = (tp + r) % n_tp
        cols = pl.ds(pl.multiple_of(q * share, share), share)
        out_part[r] = dot(act_mix, wout_v[:, cols]).astype(BF16)
    pl.semaphore_wait(barrier, n_ep - 1 + n_tp - 1)
    waits = {}
    for r in (2, 1, 3):
        waits[r] = send(
            out_part.at[r],
            out_recv.at[r - 1],
            a_send.at[r - 1],
            a_recv.at[r - 1],
            {"tp": (tp + r) % n_tp},
        )

    for name in ("routes", "gmix", "wgrp", "wexp"):
        loads[name].wait()
    route = [
        jnp.sum(
            jnp.where(
                lax.broadcasted_iota(jnp.int32, (rows, rows), 0)
                == lax.broadcasted_iota(jnp.int32, (rows, rows), 1),
                routes_v[k : k + 1, :].astype(F32),
                0.0,
            ),
            axis=1,
            keepdims=True,
        )
        for k in range(2)
    ]
    expert_id = lax.broadcasted_iota(jnp.int32, (rows, experts), 1).astype(F32)
    chosen = [(route[k] == expert_id).astype(F32) for k in range(2)]
    hits = chosen[0] + chosen[1]
    row_id = lax.broadcasted_iota(jnp.int32, (rows, rows), 0)
    col_id = lax.broadcasted_iota(jnp.int32, (rows, rows), 1)
    earlier = (row_id > col_id).astype(BF16)
    prior = dot(earlier, hits.astype(BF16))
    slot_id = lax.broadcasted_iota(jnp.int32, (rows, experts * cap), 1).astype(F32)
    places = []
    for k in range(2):
        rank = jnp.sum(prior * chosen[k], axis=1, keepdims=True)
        target = route[k] * cap + rank
        places.append((target == slot_id).astype(F32))
    dispatch_map = (places[0] + places[1]).astype(BF16)

    diagonal = (
        lax.broadcasted_iota(jnp.int32, (rows, 128), 0)
        == lax.broadcasted_iota(jnp.int32, (rows, 128), 1)
    )

    def exchange(n, columns):
        for i, column in enumerate(columns):
            stat_send[n, i : i + 1, :] = jnp.sum(
                jnp.where(diagonal, column, 0.0), axis=0, keepdims=True
            )
        for r in (2, 1, 3):
            send(
                stat_send.at[n],
                stat_recv.at[n, r - 1],
                s_send.at[n, r - 1],
                s_recv.at[n, r - 1],
                {"tp": (tp + r) % n_tp},
            )

    def received(n, count):
        for r in range(1, n_tp):
            pltpu.make_async_copy(
                stat_recv.at[n, r - 1], stat_recv.at[n, r - 1], s_recv.at[n, r - 1]
            ).wait()
        parts = [stat_send[n]] + [stat_recv[n, r - 1] for r in range(1, n_tp)]
        return [
            [
                jnp.sum(jnp.where(diagonal, part[i : i + 1, :], 0.0), axis=1, keepdims=True)
                for i in range(count)
            ]
            for part in parts
        ]

    shift = residual_scale * jnp.mean(x_v[...].astype(F32), axis=1, keepdims=True)
    base = residual_scale * x_v[:, share_at].astype(F32) - shift

    for r in range(1, n_tp):
        waits[r].wait_recv()
    mixed = out_part[0].astype(F32)
    for r in range(1, n_tp):
        mixed = mixed + out_recv[r - 1].astype(F32)
    values = base + mixed

    z_buf[...] = (
        lax.dot_general(
            dispatch_map, values.astype(BF16), (((0,), (0,)), ((), ())), preferred_element_type=F32
        )
        .reshape(n_ep, slots, share)
        .astype(BF16)
    )
    z_recv_buf[home] = z_buf[ep]
    def dispatch(k):
        for i, offset in enumerate(far if k else near):
            host = (chip + chips - offset) % chips
            if k:
                rank = (offset - NEAR - 1 + arc - wrapped(host)) % arc
                place, chunk = starts[1] + rank * CORES + core, 1 + rank // ARC
            else:
                place, chunk = i * CORES + core, 0
            for c in (1, 0):
                if offset == 0 and c == 0:
                    continue
                target = host * CORES + (core + c) % CORES
                send(
                    z_buf.at[target],
                    z_recv_buf.at[place],
                    z_send.at[k],
                    z_recv.at[chunk],
                    {"ep": target},
                )

    mean_own = jnp.mean(values, axis=1, keepdims=True)
    spread_own = jnp.sum(jnp.square(values - mean_own), axis=1, keepdims=True)
    exchange(0, [mean_own, spread_own])
    hid_v[...] = values

    def gather(k):
        wait_bytes(z_recv_buf.at[0 : remote[k]], z_recv.at[k])
        peers = ((2, opposite), (1, left), (0, right))
        for n, peer in peers:
            send(
                z_recv_buf.at[blocks[k]],
                gather_buf.at[tp, blocks[k]],
                x_send.at[k],
                x_recv.at[k, n],
                {"tp": peer},
            )
        gather_buf[tp, blocks[k]] = z_recv_buf[blocks[k]]

    def experts_of(k):
        for n in range(3):
            wait_bytes(gather_buf.at[0, blocks[k]], x_recv.at[k, n])
        if k == 0:
            for name in ("wg", "wu", "wd"):
                loads[name].wait()
        rows_k = counts[k] * slots
        parts = [gather_buf[t, blocks[k]].astype(F32).reshape(rows_k, share) for t in range(n_tp)]
        mean = sum(jnp.sum(p, axis=1, keepdims=True) for p in parts) / width
        parts = [p - mean for p in parts]
        spread = sum(jnp.sum(jnp.square(p), axis=1, keepdims=True) for p in parts) / width
        scale = lax.rsqrt(spread + norm_eps)
        lhs = jnp.concatenate(
            [
                (p * scale * gmix_v[:, t * share : (t + 1) * share]).astype(BF16)
                for t, p in enumerate(parts)
            ],
            axis=1,
        )
        slot = lax.broadcasted_iota(jnp.int32, (rows_k, 1), 0) % slots
        acts = []
        for e in range(local_experts):
            gate = dot(lhs, wg_v[e])
            up = dot(lhs, wu_v[e])
            mine = slot // cap == e
            acts.append(jnp.where(mine, jax.nn.silu(gate) * up, 0.0).astype(BF16))
        act = jnp.concatenate(acts, axis=1)
        for r in (2, 1, 3, 0):
            q = (tp + r) % n_tp
            cols = pl.ds(pl.multiple_of(q * share, share), share)
            down_part[r, sums[k]] = dot(act, wd_v[:, cols]).astype(BF16)
            if r:
                send(
                    down_part.at[r, sums[k]],
                    down_recv.at[r - 1, sums[k]],
                    d_send.at[k],
                    d_recv.at[k, r - 1],
                    {"tp": q},
                )

    def give_back(k):
        for n in range(3):
            wait_bytes(down_recv.at[n, sums[k]], d_recv.at[k, n])
        total = down_part[0, sums[k]].astype(F32)
        for n in range(3):
            total = total + down_recv[n, sums[k]].astype(F32)
        ret_send[blocks[k]] = total.reshape(counts[k], slots, share).astype(BF16)
        for i in range(counts[k] // CORES):
            if k:
                rank = (k - 1) * ARC + i
                source = (chip + NEAR + 1 + (rank + wrapped(chip)) % arc) % chips
            else:
                source = (chip + chips + near[i]) % chips
            for c in (1, 0):
                to_core = (core + c) % CORES
                if k == 0 and near[i] == 0 and c == 0:
                    ret_buf[ep] = ret_send[home]
                    continue
                send(
                    ret_send.at[starts[k] + i * CORES + to_core],
                    ret_buf.at[ep],
                    r_send.at[k],
                    r_recv,
                    {"ep": source * CORES + to_core},
                )

    def router(k):
        stats = received(0, 2)
        mean = sum(s[0] for s in stats) / n_tp
        spread = sum(s[1] + share * jnp.square(s[0] - mean) for s in stats) / width
        hidden = (hid_v[...] - mean) * lax.rsqrt(spread + norm_eps) * gmix_v[:, share_at]
        hid_v[...] = hidden
        hidden_bf = hidden.astype(BF16)

        group_logit = dot_t(hidden_bf, wgrp_v[...])
        expert_logit = dot_t(hidden_bf, wexp_v[...])
        columns = [jnp.sum(chosen[k] * expert_logit, axis=1, keepdims=True) for k in range(2)]
        columns += [group_logit[:, i : i + 1] for i in range(egroups)]
        exchange(1, columns)

    weights = []

    def route_weights(k):
        parts = received(1, 2 + egroups)
        total = [sum(p[i] for p in parts) for i in range(2 + egroups)]
        pair = [jnp.exp(total[k]) for k in range(2)]
        group_exp = [jnp.exp(total[2 + i]) for i in range(egroups)]
        group_size = experts // egroups
        picked = sum(
            jnp.where(
                (route[0] >= i * group_size) & (route[0] < (i + 1) * group_size), group_exp[i], 0.0
            )
            for i in range(egroups)
        )
        group_prob = picked / sum(group_exp)
        pair_sum = pair[0] + pair[1]
        combine_map = sum(places[k] * (pair[k] / pair_sum * group_prob) for k in range(2))
        weights.append(combine_map.astype(BF16))

    steps = {
        "D": dispatch,
        "G": gather,
        "H": router,
        "E": experts_of,
        "W": route_weights,
        "B": give_back,
    }
    for step in SCHEDULE:
        steps[step[0]](int(step[1]))

    for r in range(1, n_tp):
        wait_bytes(out_recv.at[0], a_send.at[r - 1])
        for n in range(2):
            wait_bytes(stat_send.at[n], s_send.at[n, r - 1])
    wait_bytes(z_recv_buf.at[0 : remote[0]], z_send.at[0])
    wait_bytes(z_recv_buf.at[0 : sum(remote[1:])], z_send.at[1])
    for k in range(chunks):
        wait_bytes(gather_buf.at[0:3, blocks[k]], x_send.at[k])
        wait_bytes(down_recv.at[0:3, sums[k]], d_send.at[k])
    wait_bytes(ret_buf.at[0 : n_ep - 1], r_recv)
    returned = ret_buf[...].reshape(n_ep * slots, share)
    values = residual_scale * hid_v[...] + dot(weights[0], returned)
    fin_v[...] = values.astype(BF16)
    for r in (2, 1, 3):
        send(
            fin_v, out_h.at[:, share_at], l_send, l_recv.at[r - 1], {"tp": (tp + r) % n_tp}
        )
    own_store = pltpu.make_async_copy(fin_v, out_h.at[:, share_at], o_send)
    own_store.start()
    for k in range(chunks):
        wait_bytes(ret_buf.at[0 : remote[k]], r_send.at[k])
    store.wait()
    for r in range(1, n_tp):
        wait_bytes(fin_v, l_recv.at[r - 1])
    own_store.wait()
    wait_bytes(out_recv, l_send)


def finish_kernel(
    pieces,
    raw_h,
    ns_h,
    gain_h,
    out_h,
    new_h,
    raw_v,
    ns_v,
    gain_v,
    out_v,
    load_sem,
    store_sem,
    in_sem,
    out_sem,
):
    size = ns_v.shape[0] // pieces
    raw = pltpu.make_async_copy(raw_h, raw_v, load_sem.at[0])
    gain = pltpu.make_async_copy(gain_h, gain_v, load_sem.at[1])
    raw.start()
    gain.start()
    ins, outs = [], []
    for i in range(pieces):
        part = pl.ds(i * size, size)
        ins.append(pltpu.make_async_copy(ns_h.at[part], ns_v.at[part], in_sem.at[i]))
        outs.append(pltpu.make_async_copy(ns_v.at[part], new_h.at[part], out_sem.at[i]))
        ins[i].start()
    raw.wait()
    gain.wait()
    values = raw_v[...].astype(F32)
    centred = values - jnp.mean(values, axis=1, keepdims=True)
    spread = jnp.mean(jnp.square(centred), axis=1, keepdims=True)
    out_v[...] = (centred * lax.rsqrt(spread + norm_eps) * gain_v[...]).astype(BF16)
    store = pltpu.make_async_copy(out_v, out_h, store_sem)
    store.start()
    for i in range(pieces):
        ins[i].wait()
        outs[i].start()
    for copy in outs:
        copy.wait()
    store.wait()


def per_device(
    n_ep,
    n_tp,
    x_in,
    state,
    routes,
    w_in,
    decay_rate,
    frequency,
    log_step,
    b_in,
    c_out,
    skip,
    w_out,
    gain_mix,
    w_group,
    w_expert,
    w_gate,
    w_up,
    w_down,
    gain_moe,
):
    rows, width = x_in.shape
    share = width // n_tp
    groups, entries = decay_rate.shape
    lanes = 2 * entries
    channels = skip.shape[0]
    experts = w_expert.shape[1]
    egroups = w_group.shape[1]
    local_experts, _, hidden_units = w_gate.shape
    cap = max(2, 4 * rows // experts)
    slots = local_experts * cap
    args = (
        x_in,
        state.reshape(rows * groups, lanes),
        routes.T,
        w_in,
        decay_rate,
        frequency,
        log_step.reshape(1, groups),
        b_in.reshape(channels, lanes),
        c_out.reshape(channels, lanes),
        skip.reshape(channels // lanes, lanes),
        w_out,
        gain_mix.reshape(1, width),
        w_group.T,
        w_expert.T,
        w_gate,
        w_up,
        w_down.reshape(local_experts * hidden_units, width),
    )
    dma = pltpu.SemaphoreType.DMA
    peers = n_tp - 1
    chunks = 1 + pl.cdiv(n_ep // CORES - 2 * NEAR - 1, ARC)
    scratch = [
        pltpu.VMEM((rows, width), BF16),
        pltpu.VMEM((rows * groups, lanes), F32),
        pltpu.VMEM(routes.shape[::-1], jnp.int32),
        pltpu.VMEM(w_in.shape, BF16),
        pltpu.VMEM(decay_rate.shape, F32),
        pltpu.VMEM(frequency.shape, F32),
        pltpu.VMEM((1, groups), F32),
        pltpu.VMEM((channels, lanes), F32),
        pltpu.VMEM((channels, lanes), F32),
        pltpu.VMEM((channels // lanes, lanes), F32),
        pltpu.VMEM(w_out.shape, BF16),
        pltpu.VMEM((1, width), F32),
        pltpu.VMEM((egroups, share), BF16),
        pltpu.VMEM((experts, share), BF16),
        pltpu.VMEM(w_gate.shape, BF16),
        pltpu.VMEM(w_up.shape, BF16),
        pltpu.VMEM((local_experts * hidden_units, width), BF16),
        pltpu.VMEM((rows * groups, lanes), F32),
        pltpu.VMEM((n_tp, rows, share), BF16),
        pltpu.VMEM((peers, rows, share), BF16),
        pltpu.VMEM((rows, share), F32),
        pltpu.VMEM((2, 8, 128), F32),
        pltpu.VMEM((2, peers, 8, 128), F32),
        pltpu.VMEM((n_ep, slots, share), BF16),
        pltpu.VMEM((n_ep, slots, share), BF16),
        pltpu.VMEM((n_tp, n_ep, slots, share), BF16),
        pltpu.VMEM((n_tp, n_ep * slots, share), BF16),
        pltpu.VMEM((peers, n_ep * slots, share), BF16),
        pltpu.VMEM((n_ep, slots, share), BF16),
        pltpu.VMEM((n_ep, slots, share), BF16),
        pltpu.VMEM((rows, share), BF16),
        dma((len(args),)),
        dma,
        dma((peers,)),
        dma((peers,)),
        dma((2, peers)),
        dma((2, peers)),
        dma((2,)),
        dma((chunks,)),
        dma((chunks,)),
        dma((chunks, peers)),
        dma((chunks,)),
        dma((chunks, peers)),
        dma((chunks,)),
        dma,
        dma,
        dma((peers,)),
        dma,
    ]
    any_space = pl.BlockSpec(memory_space=pl.ANY)
    raw, new_state = pl.pallas_call(
        functools.partial(layer_kernel, n_ep, n_tp),
        out_shape=(
            jax.ShapeDtypeStruct((rows, width), BF16),
            jax.ShapeDtypeStruct((rows * groups, lanes), F32),
        ),
        in_specs=[any_space] * len(args),
        out_specs=(any_space, any_space),
        scratch_shapes=scratch,
        compiler_params=pltpu.CompilerParams(
            collective_id=0, has_side_effects=True, vmem_limit_bytes=60 * 1024 * 1024
        ),
        name="layer",
    )(*args)
    pieces = 4
    out, new_state = pl.pallas_call(
        functools.partial(finish_kernel, pieces),
        out_shape=(
            jax.ShapeDtypeStruct((rows, width), BF16),
            jax.ShapeDtypeStruct((rows * groups, lanes), F32),
        ),
        in_specs=[any_space] * 3,
        out_specs=(any_space, any_space),
        scratch_shapes=[
            pltpu.VMEM((rows, width), BF16),
            pltpu.VMEM((rows * groups, lanes), F32),
            pltpu.VMEM((1, width), F32),
            pltpu.VMEM((rows, width), BF16),
            dma((2,)),
            dma,
            dma((pieces,)),
            dma((pieces,)),
        ],
        name="finish",
    )(raw, new_state, gain_moe.reshape(1, width))
    return out, new_state.reshape(state.shape)


def solution(mesh):
    in_specs = (
        P(("grp", "ep"), None),
        P(("grp", "ep"), "tp", None),
        P(("grp", "ep"), None),
        P(None, "tp"),
        P("tp", None),
        P("tp", None),
        P("tp"),
        P("tp", None, None),
        P("tp", None, None),
        P("tp"),
        P("tp", None),
        P(),
        P(),
        P(),
        P("ep", None, "tp"),
        P("ep", None, "tp"),
        P("ep", "tp", None),
        P(),
    )
    out_specs = (P(("grp", "ep"), None), P(("grp", "ep"), "tp", None))
    return jax.shard_map(
        functools.partial(per_device, mesh.shape["ep"], mesh.shape["tp"]),
        mesh=mesh,
        in_specs=in_specs,
        out_specs=out_specs,
        check_vma=False,
    )
```

```python
import functools

import jax
import jax.numpy as jnp
from jax import lax
from jax.experimental import pallas as pl
from jax.experimental.pallas import tpu as pltpu
from jax.sharding import PartitionSpec as P

residual_scale = 8.0**0.25
norm_eps = 1e-05
CORES = 2
NEAR = 1
ARC = 5
SCHEDULE = ("D0", "D1", "G0", "H0", "E0", "G1", "G2", "B0", "E1", "G3", "E2", "B1", "E3", "B2", "W0", "B3")
F32 = jnp.float32
BF16 = jnp.bfloat16
MESH = pl.DeviceIdType.MESH


def dot(a, b):
    return jnp.dot(a, b, preferred_element_type=F32)


def dot_t(a, b):
    return lax.dot_general(a, b, (((1,), (1,)), ((), ())), preferred_element_type=F32)


def layer_kernel(
    n_ep,
    n_tp,
    x_h,
    state_h,
    routes_h,
    win_h,
    decay_h,
    freq_h,
    lstep_h,
    b_h,
    c_h,
    skip_h,
    wout_h,
    gmix_h,
    wgrp_h,
    wexp_h,
    wg_h,
    wu_h,
    wd_h,
    out_h,
    ns_h,
    x_v,
    state_v,
    routes_v,
    win_v,
    decay_v,
    freq_v,
    lstep_v,
    b_v,
    c_v,
    skip_v,
    wout_v,
    gmix_v,
    wgrp_v,
    wexp_v,
    wg_v,
    wu_v,
    wd_v,
    ns_v,
    out_part,
    out_recv,
    hid_v,
    stat_send,
    stat_recv,
    z_buf,
    z_recv_buf,
    gather_buf,
    down_part,
    down_recv,
    ret_send,
    ret_buf,
    fin_v,
    load_sem,
    store_sem,
    a_send,
    a_recv,
    s_send,
    s_recv,
    z_send,
    z_recv,
    x_send,
    x_recv,
    d_send,
    d_recv,
    r_send,
    r_recv,
    l_send,
    l_recv,
    o_send,
):
    ep = lax.axis_index("ep")
    tp = lax.axis_index("tp")
    chips = n_ep // CORES
    chip = ep // CORES
    core = ep % CORES
    rows, width = x_v.shape
    share = width // n_tp
    entries = decay_v.shape[1]
    lanes = 2 * entries
    groups = decay_v.shape[0]
    group_width = b_v.shape[0] // groups
    experts = wexp_v.shape[0]
    egroups = wgrp_v.shape[0]
    local_experts = wg_v.shape[0]
    cap = z_buf.shape[1] // local_experts
    slots = z_buf.shape[1]
    arc = chips - 2 * NEAR - 1
    near = [offset for step in range(1, NEAR + 1) for offset in (step, -step)] + [0]
    far = sorted(range(NEAR + 1, chips - NEAR), key=lambda offset: abs(offset - chips // 2))
    counts = [len(near) * CORES]
    counts += [min(ARC, arc - i) * CORES for i in range(0, arc, ARC)]
    chunks = len(counts)
    starts = [sum(counts[:k]) for k in range(chunks)]
    blocks = [pl.ds(starts[k], counts[k]) for k in range(chunks)]
    sums = [pl.ds(starts[k] * slots, counts[k] * slots) for k in range(chunks)]
    remote = [counts[0] - 1] + counts[1:]
    home = len(near) * CORES - CORES + core

    def wrapped(host):
        after = (host + chips - NEAR - 1) % chips
        return (chips - NEAR - 1 - host) * (1 - after // (arc - 1))

    right, left, opposite = (tp + 1) % n_tp, (tp + n_tp - 1) % n_tp, (tp + 2) % n_tp
    share_at = pl.ds(pl.multiple_of(tp * share, share), share)

    loads = {}
    pairs = (
        ("x", x_h, x_v),
        ("win", win_h, win_v),
        ("decay", decay_h, decay_v),
        ("freq", freq_h, freq_v),
        ("lstep", lstep_h, lstep_v),
        ("b", b_h, b_v),
        ("c", c_h, c_v),
        ("state", state_h, state_v),
        ("skip", skip_h, skip_v),
        ("wout", wout_h, wout_v),
        ("gmix", gmix_h, gmix_v),
        ("routes", routes_h, routes_v),
        ("wgrp", wgrp_h.at[:, share_at], wgrp_v),
        ("wexp", wexp_h.at[:, share_at], wexp_v),
        ("wg", wg_h, wg_v),
        ("wu", wu_h, wu_v),
        ("wd", wd_h, wd_v),
    )
    for i, (name, src, dst) in enumerate(pairs):
        loads[name] = pltpu.make_async_copy(src, dst, load_sem.at[i])
        loads[name].start()

    barrier = pltpu.get_barrier_semaphore()

    def greet_ep(i, _):
        step = n_ep // 2 + jnp.where(i % 2 == 0, i // 2, -(i // 2) - 1)
        peer = (ep + step) % n_ep
        pl.semaphore_signal(barrier, inc=1, device_id={"ep": peer}, device_id_type=MESH)
        return 0

    for r in range(1, n_tp):
        pl.semaphore_signal(
            barrier, inc=1, device_id={"tp": (tp + r) % n_tp}, device_id_type=MESH
        )
    lax.fori_loop(0, n_ep - 1, greet_ep, 0, unroll=True)

    def send(src, dst, send_sem, recv_sem, target):
        copy = pltpu.make_async_remote_copy(
            src_ref=src,
            dst_ref=dst,
            send_sem=send_sem,
            recv_sem=recv_sem,
            device_id=target,
            device_id_type=MESH,
        )
        copy.start()
        return copy

    def wait_bytes(ref, sem):
        pltpu.make_async_copy(ref, ref, sem).wait()

    for name in ("decay", "freq", "lstep", "b", "c"):
        loads[name].wait()
    eye = (
        lax.broadcasted_iota(jnp.int32, (groups, groups), 0)
        == lax.broadcasted_iota(jnp.int32, (groups, groups), 1)
    )
    log_step = jnp.sum(jnp.where(eye, lstep_v[...], 0.0), axis=1, keepdims=True)
    step_size = jnp.exp(log_step)
    decay = decay_v[...]
    freq = freq_v[...]
    lam_real = -decay
    magnitude = jnp.exp(lam_real * step_size)
    angle = freq * step_size
    bar_real = magnitude * jnp.cos(angle)
    bar_imag = magnitude * jnp.sin(angle)
    minus_real = bar_real - 1.0
    modulus = lam_real * lam_real + freq * freq
    ratio_real = (minus_real * lam_real + bar_imag * freq) / modulus
    ratio_imag = (bar_imag * lam_real - minus_real * freq) / modulus
    bar_same = jnp.concatenate([bar_real, bar_real], axis=1)
    bar_cross = jnp.concatenate([-bar_imag, bar_imag], axis=1)
    ratio_same = jnp.concatenate([ratio_real, ratio_real], axis=1)
    ratio_cross = jnp.concatenate([-ratio_imag, ratio_imag], axis=1)

    loads["x"].wait()
    loads["win"].wait()
    mix_input = dot(x_v[...], win_v[...]).astype(BF16)
    loads["skip"].wait()
    loads["state"].wait()

    per_block = lanes // group_width
    block_lanes = per_block * lanes
    own_group = (
        lax.broadcasted_iota(jnp.int32, (lanes, block_lanes), 0) // group_width
        == lax.broadcasted_iota(jnp.int32, (lanes, block_lanes), 1) // lanes
    )
    sign = jnp.where(lax.broadcasted_iota(jnp.int32, (1, lanes), 1) < entries, 1.0, -1.0)
    acts = []
    for j in range(groups // per_block):
        channels = slice(j * lanes, (j + 1) * lanes)
        bars = []
        for g in range(j * per_block, (j + 1) * per_block):
            b_g = b_v[g * group_width : (g + 1) * group_width, :]
            bars.append(
                b_g * ratio_same[g : g + 1, :]
                + pltpu.roll(b_g, entries, 1) * ratio_cross[g : g + 1, :]
            )
        b_bar = jnp.concatenate(bars, axis=0)
        b_wide = jnp.where(own_group, jnp.concatenate([b_bar] * per_block, axis=1), 0.0)
        u_j = mix_input[:, channels]
        forcing = dot(u_j, b_wide.astype(BF16))
        news = []
        for i in range(per_block):
            g = j * per_block + i
            old = state_v[pl.ds(g, rows, stride=groups), :]
            new = (
                old * bar_same[g : g + 1, :]
                + pltpu.roll(old, entries, 1) * bar_cross[g : g + 1, :]
                + forcing[:, i * lanes : (i + 1) * lanes]
            )
            ns_v[pl.ds(g, rows, stride=groups), :] = new
            news.append(new.astype(BF16))
        c_j = c_v[channels, :] * sign
        c_wide = jnp.where(own_group, jnp.concatenate([c_j] * per_block, axis=1), 0.0)
        y = dot_t(jnp.concatenate(news, axis=1), c_wide.astype(BF16))
        y = y + skip_v[j : j + 1, :] * u_j.astype(F32)
        acts.append(jax.nn.gelu(y).astype(BF16))
    store = pltpu.make_async_copy(ns_v, ns_h, store_sem)
    store.start()
    act_mix = jnp.concatenate(acts, axis=1)

    loads["wout"].wait()
    for r in (2, 1, 3, 0):
        q = (tp + r) % n_tp
        cols = pl.ds(pl.multiple_of(q * share, share), share)
        out_part[r] = dot(act_mix, wout_v[:, cols]).astype(BF16)
    pl.semaphore_wait(barrier, n_ep - 1 + n_tp - 1)
    waits = {}
    for r in (2, 1, 3):
        waits[r] = send(
            out_part.at[r],
            out_recv.at[r - 1],
            a_send.at[r - 1],
            a_recv.at[r - 1],
            {"tp": (tp + r) % n_tp},
        )

    for name in ("routes", "gmix", "wgrp", "wexp"):
        loads[name].wait()
    route = [
        jnp.sum(
            jnp.where(
                lax.broadcasted_iota(jnp.int32, (rows, rows), 0)
                == lax.broadcasted_iota(jnp.int32, (rows, rows), 1),
                routes_v[k : k + 1, :].astype(F32),
                0.0,
            ),
            axis=1,
            keepdims=True,
        )
        for k in range(2)
    ]
    expert_id = lax.broadcasted_iota(jnp.int32, (rows, experts), 1).astype(F32)
    chosen = [(route[k] == expert_id).astype(F32) for k in range(2)]
    hits = chosen[0] + chosen[1]
    row_id = lax.broadcasted_iota(jnp.int32, (rows, rows), 0)
    col_id = lax.broadcasted_iota(jnp.int32, (rows, rows), 1)
    earlier = (row_id > col_id).astype(BF16)
    prior = dot(earlier, hits.astype(BF16))
    slot_id = lax.broadcasted_iota(jnp.int32, (rows, experts * cap), 1).astype(F32)
    places = []
    for k in range(2):
        rank = jnp.sum(prior * chosen[k], axis=1, keepdims=True)
        target = route[k] * cap + rank
        places.append((target == slot_id).astype(F32))
    dispatch_map = (places[0] + places[1]).astype(BF16)

    diagonal = (
        lax.broadcasted_iota(jnp.int32, (rows, 128), 0)
        == lax.broadcasted_iota(jnp.int32, (rows, 128), 1)
    )

    def exchange(n, columns):
        for i, column in enumerate(columns):
            stat_send[n, i : i + 1, :] = jnp.sum(
                jnp.where(diagonal, column, 0.0), axis=0, keepdims=True
            )
        for r in (2, 1, 3):
            send(
                stat_send.at[n],
                stat_recv.at[n, r - 1],
                s_send.at[n, r - 1],
                s_recv.at[n, r - 1],
                {"tp": (tp + r) % n_tp},
            )

    def received(n, count):
        for r in range(1, n_tp):
            pltpu.make_async_copy(
                stat_recv.at[n, r - 1], stat_recv.at[n, r - 1], s_recv.at[n, r - 1]
            ).wait()
        parts = [stat_send[n]] + [stat_recv[n, r - 1] for r in range(1, n_tp)]
        return [
            [
                jnp.sum(jnp.where(diagonal, part[i : i + 1, :], 0.0), axis=1, keepdims=True)
                for i in range(count)
            ]
            for part in parts
        ]

    shift = residual_scale * jnp.mean(x_v[...].astype(F32), axis=1, keepdims=True)
    base = residual_scale * x_v[:, share_at].astype(F32) - shift

    for r in range(1, n_tp):
        waits[r].wait_recv()
    mixed = out_part[0].astype(F32)
    for r in range(1, n_tp):
        mixed = mixed + out_recv[r - 1].astype(F32)
    values = base + mixed

    z_buf[...] = (
        lax.dot_general(
            dispatch_map, values.astype(BF16), (((0,), (0,)), ((), ())), preferred_element_type=F32
        )
        .reshape(n_ep, slots, share)
        .astype(BF16)
    )
    z_recv_buf[home] = z_buf[ep]
    def dispatch(k):
        for i, offset in enumerate(far if k else near):
            host = (chip + chips - offset) % chips
            if k:
                rank = (offset - NEAR - 1 + arc - wrapped(host)) % arc
                place, chunk = starts[1] + rank * CORES + core, 1 + rank // ARC
            else:
                place, chunk = i * CORES + core, 0
            for c in (1, 0):
                if offset == 0 and c == 0:
                    continue
                target = host * CORES + (core + c) % CORES
                send(
                    z_buf.at[target],
                    z_recv_buf.at[place],
                    z_send.at[k],
                    z_recv.at[chunk],
                    {"ep": target},
                )

    mean_own = jnp.mean(values, axis=1, keepdims=True)
    spread_own = jnp.sum(jnp.square(values - mean_own), axis=1, keepdims=True)
    exchange(0, [mean_own, spread_own])
    hid_v[...] = values

    def gather(k):
        wait_bytes(z_recv_buf.at[0 : remote[k]], z_recv.at[k])
        peers = ((2, opposite), (1, left), (0, right))
        for n, peer in peers:
            send(
                z_recv_buf.at[blocks[k]],
                gather_buf.at[tp, blocks[k]],
                x_send.at[k],
                x_recv.at[k, n],
                {"tp": peer},
            )
        gather_buf[tp, blocks[k]] = z_recv_buf[blocks[k]]

    def experts_of(k):
        for n in range(3):
            wait_bytes(gather_buf.at[0, blocks[k]], x_recv.at[k, n])
        if k == 0:
            for name in ("wg", "wu", "wd"):
                loads[name].wait()
        rows_k = counts[k] * slots
        parts = [gather_buf[t, blocks[k]].astype(F32).reshape(rows_k, share) for t in range(n_tp)]
        mean = sum(jnp.sum(p, axis=1, keepdims=True) for p in parts) / width
        parts = [p - mean for p in parts]
        spread = sum(jnp.sum(jnp.square(p), axis=1, keepdims=True) for p in parts) / width
        scale = lax.rsqrt(spread + norm_eps)
        lhs = jnp.concatenate(
            [
                (p * scale * gmix_v[:, t * share : (t + 1) * share]).astype(BF16)
                for t, p in enumerate(parts)
            ],
            axis=1,
        )
        slot = lax.broadcasted_iota(jnp.int32, (rows_k, 1), 0) % slots
        acts = []
        for e in range(local_experts):
            gate = dot(lhs, wg_v[e])
            up = dot(lhs, wu_v[e])
            mine = slot // cap == e
            acts.append(jnp.where(mine, jax.nn.silu(gate) * up, 0.0).astype(BF16))
        act = jnp.concatenate(acts, axis=1)
        for r in (2, 1, 3, 0):
            q = (tp + r) % n_tp
            cols = pl.ds(pl.multiple_of(q * share, share), share)
            down_part[r, sums[k]] = dot(act, wd_v[:, cols]).astype(BF16)
            if r:
                send(
                    down_part.at[r, sums[k]],
                    down_recv.at[r - 1, sums[k]],
                    d_send.at[k],
                    d_recv.at[k, r - 1],
                    {"tp": q},
                )

    def give_back(k):
        for n in range(3):
            wait_bytes(down_recv.at[n, sums[k]], d_recv.at[k, n])
        total = down_part[0, sums[k]].astype(F32)
        for n in range(3):
            total = total + down_recv[n, sums[k]].astype(F32)
        ret_send[blocks[k]] = total.reshape(counts[k], slots, share).astype(BF16)
        for i in range(counts[k] // CORES):
            if k:
                rank = (k - 1) * ARC + i
                source = (chip + NEAR + 1 + (rank + wrapped(chip)) % arc) % chips
            else:
                source = (chip + chips + near[i]) % chips
            for c in (1, 0):
                to_core = (core + c) % CORES
                if k == 0 and near[i] == 0 and c == 0:
                    ret_buf[ep] = ret_send[home]
                    continue
                send(
                    ret_send.at[starts[k] + i * CORES + to_core],
                    ret_buf.at[ep],
                    r_send.at[k],
                    r_recv,
                    {"ep": source * CORES + to_core},
                )

    def router(k):
        stats = received(0, 2)
        mean = sum(s[0] for s in stats) / n_tp
        spread = sum(s[1] + share * jnp.square(s[0] - mean) for s in stats) / width
        hidden = (hid_v[...] - mean) * lax.rsqrt(spread + norm_eps) * gmix_v[:, share_at]
        hid_v[...] = hidden
        hidden_bf = hidden.astype(BF16)

        group_logit = dot_t(hidden_bf, wgrp_v[...])
        expert_logit = dot_t(hidden_bf, wexp_v[...])
        columns = [jnp.sum(chosen[k] * expert_logit, axis=1, keepdims=True) for k in range(2)]
        columns += [group_logit[:, i : i + 1] for i in range(egroups)]
        exchange(1, columns)

    weights = []

    def route_weights(k):
        parts = received(1, 2 + egroups)
        total = [sum(p[i] for p in parts) for i in range(2 + egroups)]
        pair = [jnp.exp(total[k]) for k in range(2)]
        group_exp = [jnp.exp(total[2 + i]) for i in range(egroups)]
        group_size = experts // egroups
        picked = sum(
            jnp.where(
                (route[0] >= i * group_size) & (route[0] < (i + 1) * group_size), group_exp[i], 0.0
            )
            for i in range(egroups)
        )
        group_prob = picked / sum(group_exp)
        pair_sum = pair[0] + pair[1]
        combine_map = sum(places[k] * (pair[k] / pair_sum * group_prob) for k in range(2))
        weights.append(combine_map.astype(BF16))

    steps = {
        "D": dispatch,
        "G": gather,
        "H": router,
        "E": experts_of,
        "W": route_weights,
        "B": give_back,
    }
    for step in SCHEDULE:
        steps[step[0]](int(step[1]))

    for r in range(1, n_tp):
        wait_bytes(out_recv.at[0], a_send.at[r - 1])
        for n in range(2):
            wait_bytes(stat_send.at[n], s_send.at[n, r - 1])
    wait_bytes(z_recv_buf.at[0 : remote[0]], z_send.at[0])
    wait_bytes(z_recv_buf.at[0 : sum(remote[1:])], z_send.at[1])
    for k in range(chunks):
        wait_bytes(gather_buf.at[0:3, blocks[k]], x_send.at[k])
        wait_bytes(down_recv.at[0:3, sums[k]], d_send.at[k])
    wait_bytes(ret_buf.at[0 : n_ep - 1], r_recv)
    returned = ret_buf[...].reshape(n_ep * slots, share)
    values = residual_scale * hid_v[...] + dot(weights[0], returned)
    fin_v[...] = values.astype(BF16)
    for r in (2, 1, 3):
        send(
            fin_v, out_h.at[:, share_at], l_send, l_recv.at[r - 1], {"tp": (tp + r) % n_tp}
        )
    own_store = pltpu.make_async_copy(fin_v, out_h.at[:, share_at], o_send)
    own_store.start()
    for k in range(chunks):
        wait_bytes(ret_buf.at[0 : remote[k]], r_send.at[k])
    store.wait()
    for r in range(1, n_tp):
        wait_bytes(fin_v, l_recv.at[r - 1])
    own_store.wait()
    wait_bytes(out_recv, l_send)


def finish_kernel(
    pieces,
    raw_h,
    ns_h,
    gain_h,
    out_h,
    new_h,
    raw_v,
    ns_v,
    gain_v,
    out_v,
    load_sem,
    store_sem,
    in_sem,
    out_sem,
):
    size = ns_v.shape[0] // pieces
    raw = pltpu.make_async_copy(raw_h, raw_v, load_sem.at[0])
    gain = pltpu.make_async_copy(gain_h, gain_v, load_sem.at[1])
    raw.start()
    gain.start()
    ins, outs = [], []
    for i in range(pieces):
        part = pl.ds(i * size, size)
        ins.append(pltpu.make_async_copy(ns_h.at[part], ns_v.at[part], in_sem.at[i]))
        outs.append(pltpu.make_async_copy(ns_v.at[part], new_h.at[part], out_sem.at[i]))
        ins[i].start()
    raw.wait()
    gain.wait()
    values = raw_v[...].astype(F32)
    centred = values - jnp.mean(values, axis=1, keepdims=True)
    spread = jnp.mean(jnp.square(centred), axis=1, keepdims=True)
    out_v[...] = (centred * lax.rsqrt(spread + norm_eps) * gain_v[...]).astype(BF16)
    store = pltpu.make_async_copy(out_v, out_h, store_sem)
    store.start()
    for i in range(pieces):
        ins[i].wait()
        outs[i].start()
    for copy in outs:
        copy.wait()
    store.wait()


def per_device(
    n_ep,
    n_tp,
    x_in,
    state,
    routes,
    w_in,
    decay_rate,
    frequency,
    log_step,
    b_in,
    c_out,
    skip,
    w_out,
    gain_mix,
    w_group,
    w_expert,
    w_gate,
    w_up,
    w_down,
    gain_moe,
):
    rows, width = x_in.shape
    share = width // n_tp
    groups, entries = decay_rate.shape
    lanes = 2 * entries
    channels = skip.shape[0]
    experts = w_expert.shape[1]
    egroups = w_group.shape[1]
    local_experts, _, hidden_units = w_gate.shape
    cap = max(2, 4 * rows // experts)
    slots = local_experts * cap
    args = (
        x_in,
        state.reshape(rows * groups, lanes),
        routes.T,
        w_in,
        decay_rate,
        frequency,
        log_step.reshape(1, groups),
        b_in.reshape(channels, lanes),
        c_out.reshape(channels, lanes),
        skip.reshape(channels // lanes, lanes),
        w_out,
        gain_mix.reshape(1, width),
        w_group.T,
        w_expert.T,
        w_gate,
        w_up,
        w_down.reshape(local_experts * hidden_units, width),
    )
    dma = pltpu.SemaphoreType.DMA
    peers = n_tp - 1
    chunks = 1 + pl.cdiv(n_ep // CORES - 2 * NEAR - 1, ARC)
    scratch = [
        pltpu.VMEM((rows, width), BF16),
        pltpu.VMEM((rows * groups, lanes), F32),
        pltpu.VMEM(routes.shape[::-1], jnp.int32),
        pltpu.VMEM(w_in.shape, BF16),
        pltpu.VMEM(decay_rate.shape, F32),
        pltpu.VMEM(frequency.shape, F32),
        pltpu.VMEM((1, groups), F32),
        pltpu.VMEM((channels, lanes), F32),
        pltpu.VMEM((channels, lanes), F32),
        pltpu.VMEM((channels // lanes, lanes), F32),
        pltpu.VMEM(w_out.shape, BF16),
        pltpu.VMEM((1, width), F32),
        pltpu.VMEM((egroups, share), BF16),
        pltpu.VMEM((experts, share), BF16),
        pltpu.VMEM(w_gate.shape, BF16),
        pltpu.VMEM(w_up.shape, BF16),
        pltpu.VMEM((local_experts * hidden_units, width), BF16),
        pltpu.VMEM((rows * groups, lanes), F32),
        pltpu.VMEM((n_tp, rows, share), BF16),
        pltpu.VMEM((peers, rows, share), BF16),
        pltpu.VMEM((rows, share), F32),
        pltpu.VMEM((2, 8, 128), F32),
        pltpu.VMEM((2, peers, 8, 128), F32),
        pltpu.VMEM((n_ep, slots, share), BF16),
        pltpu.VMEM((n_ep, slots, share), BF16),
        pltpu.VMEM((n_tp, n_ep, slots, share), BF16),
        pltpu.VMEM((n_tp, n_ep * slots, share), BF16),
        pltpu.VMEM((peers, n_ep * slots, share), BF16),
        pltpu.VMEM((n_ep, slots, share), BF16),
        pltpu.VMEM((n_ep, slots, share), BF16),
        pltpu.VMEM((rows, share), BF16),
        dma((len(args),)),
        dma,
        dma((peers,)),
        dma((peers,)),
        dma((2, peers)),
        dma((2, peers)),
        dma((2,)),
        dma((chunks,)),
        dma((chunks,)),
        dma((chunks, peers)),
        dma((chunks,)),
        dma((chunks, peers)),
        dma((chunks,)),
        dma,
        dma,
        dma((peers,)),
        dma,
    ]
    any_space = pl.BlockSpec(memory_space=pl.ANY)
    raw, new_state = pl.pallas_call(
        functools.partial(layer_kernel, n_ep, n_tp),
        out_shape=(
            jax.ShapeDtypeStruct((rows, width), BF16),
            jax.ShapeDtypeStruct((rows * groups, lanes), F32),
        ),
        in_specs=[any_space] * len(args),
        out_specs=(any_space, any_space),
        scratch_shapes=scratch,
        compiler_params=pltpu.CompilerParams(
            collective_id=0, has_side_effects=True, vmem_limit_bytes=60 * 1024 * 1024
        ),
        name="layer",
    )(*args)
    pieces = 4
    out, new_state = pl.pallas_call(
        functools.partial(finish_kernel, pieces),
        out_shape=(
            jax.ShapeDtypeStruct((rows, width), BF16),
            jax.ShapeDtypeStruct((rows * groups, lanes), F32),
        ),
        in_specs=[any_space] * 3,
        out_specs=(any_space, any_space),
        scratch_shapes=[
            pltpu.VMEM((rows, width), BF16),
            pltpu.VMEM((rows * groups, lanes), F32),
            pltpu.VMEM((1, width), F32),
            pltpu.VMEM((rows, width), BF16),
            dma((2,)),
            dma,
            dma((pieces,)),
            dma((pieces,)),
        ],
        name="finish",
    )(raw, new_state, gain_moe.reshape(1, width))
    return out, new_state.reshape(state.shape)


def solution(mesh):
    in_specs = (
        P(("grp", "ep"), None),
        P(("grp", "ep"), "tp", None),
        P(("grp", "ep"), None),
        P(None, "tp"),
        P("tp", None),
        P("tp", None),
        P("tp"),
        P("tp", None, None),
        P("tp", None, None),
        P("tp"),
        P("tp", None),
        P(),
        P(),
        P(),
        P("ep", None, "tp"),
        P("ep", None, "tp"),
        P("ep", "tp", None),
        P(),
    )
    out_specs = (P(("grp", "ep"), None), P(("grp", "ep"), "tp", None))
    return jax.shard_map(
        functools.partial(per_device, mesh.shape["ep"], mesh.shape["tp"]),
        mesh=mesh,
        in_specs=in_specs,
        out_specs=out_specs,
        check_vma=False,
    )
```
